768 devices in a mesh: sp: 96 (over z, y), tp: 8 (over x, core).
Axes of the slice: x: 4, y: 8, z: 12, core: 2. Of those that a mesh axis runs over, the one named last changes fastest.
Arguments:
- normalized_sequence: bfloat16 [24576, 3072], P('sp', 'tp'), may hold values from -6 to 6
- probe_projection: bfloat16 [3072, 1024], P(None, 'tp'), may hold values from -0.109375 to 0.109375
- payload_array: bfloat16 [24576, 1024], P('sp', 'tp'), may hold values from -6 to 6
- onward_retain_scores: bfloat16 [24576, 1024], P('sp', 'tp'), may hold values from -5 to 5
- reverse_retain_scores: bfloat16 [24576, 1024], P('sp', 'tp'), may hold values from -5 to 5
- retention_slack: float32 [2, 1024], P(None, 'tp'), as said below
- additional_decay: float32 [2, 24576, 8], P(None, 'sp', 'tp'), may hold values from -1.38 to 0, as said below
- rescale_weights: float32 [1024], P('tp'), may hold values from 0.1 to 1.9
- result_cotangent: bfloat16 [24576, 1024], P('sp', 'tp'), may hold values from -6 to 6
Outputs:
- query_pre_grad: bfloat16 [24576, 1024], P('sp', 'tp')
- gate_fwd_grad: float32 [24576, 1024], P('sp', 'tp')
- gate_bwd_grad: float32 [24576, 1024], P('sp', 'tp')
- value_grad: bfloat16 [24576, 1024], P('sp', 'tp')
- query_weight_grad: float32 [3072, 1024], P('sp', 'tp')
The draws below stay inside these ranges and needn't reach their ends.
Inputs may be any that keep to these rules, and one draw needn't show every extreme that they name: `retention_slack`: every entry is positive. `additional_decay`: zero except at a few positions.
All inputs are finite; a program needn't handle non-finite values.
Results may differ from the reference program's by a relative error of at most 0.025.
Values may be sent and summed in bfloat16 or wider, within the bound.
A program may use at most 64 MiB of HBM per device.

```python
import math
import jax
import jax.numpy as jnp
from jax import lax

D = 3072
HEADS = 8
ATTENTION_WIDTH = 128
BLOCK = 128
TOK_DEV = 256
TOKENS = 24576
HW = 1024


def draw_retention_slack(key, part):
    chooser, slow_key, fast_key = jax.random.split(key, 3)
    fast_share = 0.5
    fast_heads = jax.random.bernoulli(chooser, fast_share, (2, HEADS, 1))
    slow_gap = jnp.exp(jax.random.uniform(slow_key, (2, HEADS, ATTENTION_WIDTH), jnp.float32, math.log(0.3), math.log(1.5))) / TOKENS
    fast_gap = jnp.exp(jax.random.uniform(fast_key, (2, HEADS, ATTENTION_WIDTH), jnp.float32, math.log(0.02), math.log(0.06)))
    return jnp.where(fast_heads, fast_gap, slow_gap).reshape(2, HEADS * ATTENTION_WIDTH)


def draw_additional_decay(key, part):
    place_key, depth_key = jax.random.split(key)
    spike_places = jax.random.randint(place_key, (2, 2, HEADS), 0, TOKENS)
    depth_levels = jax.random.uniform(depth_key, (2, 2, HEADS), jnp.float32, 0.22, 0.69)
    token_positions = jnp.arange(TOKENS)[None, :, None]
    total_output = jnp.zeros((2, TOKENS, HEADS), jnp.float32)
    for spike_index in range(2):
        spike_hits = token_positions == spike_places[:, spike_index][:, None, :]
        total_output = total_output - jnp.where(spike_hits, depth_levels[:, spike_index][:, None, :], 0.0)
    return total_output


def shifted_gates(key, salt):
    noise_key, shift_key = jax.random.split(jax.random.fold_in(key, salt))
    noise = jax.random.truncated_normal(noise_key, -4.0, 4.0, (TOKENS, HEADS * ATTENTION_WIDTH), jnp.float32)
    shifts = jax.random.uniform(shift_key, (TOKENS // TOK_DEV, 1, HEADS, 1), jnp.float32, -1.0, 1.0)
    shifted = noise.reshape(TOKENS // TOK_DEV, TOK_DEV, HEADS, ATTENTION_WIDTH) + shifts
    return shifted.reshape(TOKENS, HEADS * ATTENTION_WIDTH)


def draw_onward_retain_scores(key, part):
    return shifted_gates(key, 11).astype(jnp.bfloat16)


def draw_reverse_retain_scores(key, part):
    return shifted_gates(key, 12).astype(jnp.bfloat16)


def shard_levels(own_key, shape, pieces, low, largest):
    def one(dim, parts):
        draws = jax.random.uniform(jax.random.fold_in(jax.random.fold_in(own_key, 6), dim), (parts,), jnp.float32, low / len(pieces), largest / len(pieces))
        return jnp.repeat(jnp.exp(draws), shape[dim] // parts).reshape((-1,) + (1,) * (len(shape) - dim - 1))

    factor_of = one(*pieces[0])
    for cut in pieces[1:]:
        factor_of = factor_of * one(*cut)
    return factor_of


def bell_draw(key, shape, width, limit, shards=(), kind=jnp.bfloat16):
    result = jax.random.normal(key, shape, jnp.float32) * width
    if len(shards) > 0:
        result = shard_levels(key, shape, shards, -0.22, 0.18) * result
    return jnp.clip(result, min=-limit, max=limit).astype(kind)


def setup_inputs(seed: int = 0) -> dict:
    seeds = jax.random.split(jax.random.key(seed), 10)
    return {
        "normalized_sequence": bell_draw(seeds[0], (TOKENS, D), 1.0, 6.0, ((0, 96), (1, 8))),
        "probe_projection": bell_draw(seeds[1], (D, HW), D ** -0.5, 0.109375, ((1, 8),)),
        "payload_array": bell_draw(seeds[2], (TOKENS, HW), 1.0, 6.0, ((0, 96), (1, 8))),
        "onward_retain_scores": draw_onward_retain_scores(jax.random.fold_in(seeds[9], 71), 0),
        "reverse_retain_scores": draw_reverse_retain_scores(jax.random.fold_in(seeds[9], 71), 0),
        "retention_slack": draw_retention_slack(jax.random.fold_in(seeds[9], 71), 0),
        "additional_decay": draw_additional_decay(jax.random.fold_in(seeds[9], 71), 0),
        "rescale_weights": jnp.clip(1.0 + 0.18 * jax.random.normal(seeds[7], (HW,), jnp.float32), 0.1, 1.9),
        "result_cotangent": bell_draw(seeds[8], (TOKENS, HW), 1.0, 6.0, ((0, 96), (1, 8))),
    }


epsilon = 1e-06

def recurrence(queries, key_matrix, values, forget_logarithm, initial):
    length, attention_count = (queries.shape[0], queries.shape[1])
    block_count = length // BLOCK
    within_mask = jnp.tril(jnp.ones((BLOCK, BLOCK), bool))
    highest = lax.Precision.HIGHEST

    def advance(carried_state, segment):
        query_seg, key_seg, value_seg, forget_seg = segment
        running = jnp.cumsum(forget_seg, axis=0)
        query_dec = query_seg * jnp.exp(running)
        key_dec = key_seg * jnp.exp(-running)
        scores = jnp.einsum('thd,shd->hts', query_dec, key_dec, precision=highest)
        scores = jnp.where(within_mask[None], scores, 0.0)
        output = jnp.einsum('hts,she->the', scores, value_seg, precision=highest)
        output = output + jnp.einsum('thd,hde->the', query_dec, carried_state, precision=highest)
        closing = running[-1]
        carried_state = jnp.exp(closing)[:, :, None] * carried_state + jnp.einsum('shd,she->hde', key_seg * jnp.exp(closing[None] - running), value_seg, precision=highest)
        return (carried_state, output)
    blocks = tuple((member.reshape((block_count, BLOCK) + member.shape[1:]) for member in (queries, key_matrix, values, forget_logarithm)))
    final_state, outputs = lax.scan(jax.checkpoint(advance), initial, blocks)
    return outputs.reshape(length, attention_count, values.shape[2])

def retention_update(gate_input_rows, margin_row, spike_column):
    key_matrix = margin_row * jax.nn.sigmoid(-gate_input_rows)
    forget_logarithm = jnp.log1p(-key_matrix) + spike_column[:, :, None]
    return (key_matrix, forget_logarithm)

def blending_update(probe_before_activation, onward_raw_scores, reverse_raw_scores, payload_entries, onward_seed_memory, reverse_seed_memory, retention_slack, additional_decay, rescale_weights):
    length = probe_before_activation.shape[0]
    attention_count = probe_before_activation.shape[1] // ATTENTION_WIDTH

    def partition_attention(array):
        return array.reshape(length, attention_count, ATTENTION_WIDTH)
    queries = partition_attention(jax.nn.silu(probe_before_activation) * ATTENTION_WIDTH ** (-0.5))
    values = partition_attention(payload_entries)
    onward_addressing, onward_retention = retention_update(partition_attention(onward_raw_scores), retention_slack[0].reshape(attention_count, ATTENTION_WIDTH), additional_decay[0])
    reverse_addressing, reverse_retention = retention_update(partition_attention(reverse_raw_scores), retention_slack[1].reshape(attention_count, ATTENTION_WIDTH), additional_decay[1])
    out_fwd = recurrence(queries, onward_addressing, values, onward_retention, onward_seed_memory)
    out_bwd = jnp.flip(recurrence(jnp.flip(queries, 0), jnp.flip(reverse_addressing, 0), jnp.flip(values, 0), jnp.flip(reverse_retention, 0), reverse_seed_memory), 0)
    mixed = out_fwd + out_bwd
    normed = mixed * lax.rsqrt(lax.optimization_barrier(jnp.mean(mixed * mixed, axis=-1, keepdims=True)) + epsilon)
    normed = normed * rescale_weights.reshape(attention_count, ATTENTION_WIDTH)
    return normed.reshape(length, attention_count * ATTENTION_WIDTH)

def reference(normalized_sequence, probe_projection, payload_array, onward_retain_scores, reverse_retain_scores, retention_slack, additional_decay, rescale_weights, result_cotangent):
    probe_before_activation = jnp.dot(normalized_sequence, probe_projection, preferred_element_type=jnp.float32).astype(jnp.bfloat16)
    attention_count = probe_projection.shape[1] // ATTENTION_WIDTH
    blank_memory = jnp.zeros((attention_count, ATTENTION_WIDTH, ATTENTION_WIDTH), jnp.float32)

    def forward(probe_raw_scores, onward_raw_scores, reverse_raw_scores, payload_entries):
        return blending_update(probe_raw_scores, onward_raw_scores, reverse_raw_scores, payload_entries, blank_memory, blank_memory, retention_slack, additional_decay, rescale_weights)
    unused, pullback = jax.vjp(forward, probe_before_activation.astype(jnp.float32), onward_retain_scores.astype(jnp.float32), reverse_retain_scores.astype(jnp.float32), payload_array.astype(jnp.float32))
    grad_query, grad_fwd, grad_bwd, grad_value = pullback(result_cotangent.astype(jnp.float32))
    query_pre_grad = grad_query.astype(jnp.bfloat16)
    weight_grad = lax.dot_general(normalized_sequence, query_pre_grad, (((0,), (0,)), ((), ())), preferred_element_type=jnp.float32)
    return (query_pre_grad, grad_fwd, grad_bwd, grad_value.astype(jnp.bfloat16), weight_grad)
```

```python
import functools

import jax
import jax.numpy as jnp
from jax import lax
from jax.experimental import pallas as pl
from jax.experimental.pallas import tpu as pltpu
from jax.sharding import Mesh
from jax.sharding import PartitionSpec as P

WIDTH = 128
HALF = 128
NZ, NY = 12, 8
EPS = 1e-6
MESH_ID = pl.DeviceIdType.MESH
F32, BF16 = jnp.float32, jnp.bfloat16

NN = (((1,), (0,)), ((), ()))
NT = (((1,), (1,)), ((), ()))
TN = (((0,), (0,)), ((), ()))


def dot(a, b, dims):
    a, b = (p if isinstance(p, tuple) else (p,) for p in (a, b))
    total = lax.dot_general(a[0], b[0], dims, preferred_element_type=F32)
    for tail in a[1:]:
        total += lax.dot_general(tail, b[0], dims, preferred_element_type=F32)
    for tail in b[1:]:
        total += lax.dot_general(a[0], tail, dims, preferred_element_type=F32)
    return total


def pair_of(x):
    head = x.astype(BF16)
    return head, (x - head.astype(F32)).astype(BF16)


def cut(pair, *at):
    return tuple(part[at] for part in pair)


def pieces(x, count):
    parts = []
    for _ in range(count):
        part = x.astype(BF16)
        parts.append(part)
        x = x - part.astype(F32)
    return parts


def summed(triangle, x, count):
    return sum(dot(triangle, part, NN) for part in pieces(x, count))


def both(x):
    return jnp.concatenate([x, x], axis=1)


def swapped(x):
    return jnp.concatenate([x[:, WIDTH:], x[:, :WIDTH]], axis=1)


def remote(src, dst, send, recv, peer):
    return pltpu.make_async_remote_copy(
        src_ref=src, dst_ref=dst, send_sem=send, recv_sem=recv, device_id=peer, device_id_type=MESH_ID
    )


def kernel(
    nz, ny, nt,
    x_ref, w_ref, v_ref, gf_ref, gb_ref, slack_ref, extra_ref, scale_ref, cot_ref,
    dq_ref, dgf_ref, dgb_ref, dv_ref, dw_ref,
    xall, xturn, dec_y, dec_z, dec_line,
    out1, in1, mid1, got1, back1, state1,
    out2, in2, mid2, got2, back2, state2,
    wg, wg_in, wg_mid, wg_got,
    x_send, x_recv, dy_send, dy_recv, dz_send, dz_recv,
    a1s, a1r, b1s, b1r, c1s, c1r,
    a2s, a2r, b2s, b2r, c2s, c2r,
    ws, wr, zs, zr,
):
    z, y, t = lax.axis_index("sp_0"), lax.axis_index("sp_1"), lax.axis_index("tp")
    rows = WIDTH // ny
    length = v_ref.shape[0]
    width_in = x_ref.shape[1]

    def far_first(n):
        return sorted(range(1, n), key=lambda o: -min(o, n - o))

    def at_y(o):
        return lax.rem(y + o, ny)

    def at_z(o):
        return lax.rem(z + o, nz)

    partner = t + 1 - 2 * lax.rem(t, 2)
    chips = [lax.rem(t + 2 * o, nt) for o in far_first(nt // 2)]

    barrier = pltpu.get_barrier_semaphore()
    count = 0
    for o in range(1, nz):
        pl.semaphore_signal(barrier, inc=1, device_id={"sp_0": at_z(o)}, device_id_type=MESH_ID)
        count += 1
    for o in range(1, ny):
        pl.semaphore_signal(barrier, inc=1, device_id={"sp_1": at_y(o)}, device_id_type=MESH_ID)
        count += 1
    for k in [partner] + chips:
        pl.semaphore_signal(barrier, inc=1, device_id={"tp": k}, device_id_type=MESH_ID)
        count += 1

    sent = []

    def send(src, dst, send_sem, recv_sem, peer):
        copy = remote(src, dst, send_sem, recv_sem, peer)
        copy.start()
        sent.append(copy)

    def arrived(dst, send_sem, recv_sem, peer):
        remote(dst, dst, send_sem, recv_sem, peer).wait_recv()

    pre = jnp.concatenate([gf_ref[...], gb_ref[...]], axis=1).astype(F32)
    slack = jnp.concatenate([slack_ref[0:1, :], slack_ref[1:2, :]], axis=1)
    gate = jax.nn.sigmoid(-pre)
    key = slack * gate
    forget = jnp.log1p(-key)
    row_id = lax.broadcasted_iota(jnp.int32, (length, length), 0)
    col_id = lax.broadcasted_iota(jnp.int32, (length, length), 1)
    lower = row_id >= col_id
    upper = row_id <= col_id
    lower_ones = jnp.where(lower, 1.0, 0.0).astype(BF16)
    upper_ones = jnp.where(upper, 1.0, 0.0).astype(BF16)
    spikes_f = jnp.sum(jnp.where(lower, extra_ref[0], 0.0), axis=1, keepdims=True)
    spikes_b = jnp.sum(jnp.where(upper, extra_ref[1], 0.0), axis=1, keepdims=True)
    run = jnp.concatenate(
        [
            summed(lower_ones, forget[:, :WIDTH], 3) + spikes_f,
            summed(upper_ones, forget[:, WIDTH:], 3) + spikes_b,
        ],
        axis=1,
    )
    closing = jnp.concatenate([run[length - 1 :, :WIDTH], run[0:1, WIDTH:]], axis=1)
    to_end = jnp.exp(closing - run)
    key_end = (key * to_end).astype(BF16)
    v = v_ref[...]
    local = dot(v, key_end, TN)
    out1[...] = local.astype(BF16).reshape(ny, rows, 2 * WIDTH)
    dec_y[pl.ds(y, 1)] = closing[None]
    in1[pl.ds(y, 1)] = out1[pl.ds(y, 1)]

    pl.semaphore_wait(barrier, count)

    def first_phase(out, into, ss, rs):
        for o in far_first(ny):
            k = at_y(o)
            send(out.at[k], into.at[y], ss.at[o], rs.at[y], {"sp_1": k})

    def first_wait(into, ss, rs):
        for o in range(1, ny):
            k = at_y(o)
            arrived(into.at[k], ss.at[o], rs.at[k], {"sp_1": k})

    def line_fold(into, decays):
        up, down = [None] * ny, [None] * ny
        total = jnp.zeros((rows, WIDTH), F32)
        for k in range(ny):
            up[k] = total
            total = jnp.exp(decays[k][:, :WIDTH]) * total + into[k, :, :WIDTH].astype(F32)
        total_up = total
        total = jnp.zeros((rows, WIDTH), F32)
        for k in reversed(range(ny)):
            down[k] = total
            total = jnp.exp(decays[k][:, WIDTH:]) * total + into[k, :, WIDTH:].astype(F32)
        return up, down, total_up, total

    def second_phase(mid, got, totals, ss, rs):
        mid[0] = totals[0].astype(BF16)
        mid[1] = totals[1].astype(BF16)
        got[pl.ds(z, 1)] = jnp.zeros((1, rows, WIDTH), BF16)
        for o in far_first(nz):
            k = at_z(o)
            side = jnp.where(k > z, 0, 1)
            send(mid.at[side], got.at[z], ss.at[o], rs.at[z], {"sp_0": k})

    def second_wait(got, ss, rs):
        for o in range(1, nz):
            k = at_z(o)
            arrived(got.at[k], ss.at[o], rs.at[k], {"sp_0": k})

    def line_entry(got, decays):
        above = jnp.zeros((rows, WIDTH), F32)
        for k in range(nz):
            new = jnp.exp(decays[k][:, :WIDTH]) * above + got[k].astype(F32)
            above = jnp.where(k < z, new, above)
        below = jnp.zeros((rows, WIDTH), F32)
        for k in reversed(range(nz)):
            new = jnp.exp(decays[k][:, WIDTH:]) * below + got[k].astype(F32)
            below = jnp.where(k > z, new, below)
        return above, below

    def third_phase(back, state, entry, prefixes, decays, ss, rs):
        above, below = entry
        up, down = prefixes
        gone = jnp.zeros((1, WIDTH), F32)
        first = []
        for k in range(ny):
            first.append(jnp.exp(gone) * above + up[k])
            gone = gone + decays[k][:, :WIDTH]
        gone = jnp.zeros((1, WIDTH), F32)
        second = [None] * ny
        for k in reversed(range(ny)):
            second[k] = jnp.exp(gone) * below + down[k]
            gone = gone + decays[k][:, WIDTH:]
        for k in range(ny):
            back[k] = jnp.concatenate([first[k], second[k]], axis=1).astype(BF16)
        here = pl.ds(pl.multiple_of(y * rows, rows), rows)
        for o in far_first(ny):
            k = at_y(o)
            send(back.at[k], state.at[here, :], ss.at[o], rs.at[y], {"sp_1": k})
        state[here, :] = back[pl.ds(y, 1)].reshape(rows, 2 * WIDTH)

    def third_wait(state, ss, rs):
        for o in range(1, ny):
            k = at_y(o)
            there = pl.ds(pl.multiple_of(k * rows, rows), rows)
            arrived(state.at[there, :], ss.at[o], rs.at[k], {"sp_1": k})

    for o in far_first(ny):
        k = at_y(o)
        send(dec_y.at[y], dec_y.at[y], dy_send.at[o], dy_recv.at[y], {"sp_1": k})
    first_phase(out1, in1, a1s, a1r)
    for i, k in enumerate(chips):
        send(x_ref, xall.at[t], x_send.at[i], x_recv.at[t], {"tp": k})
    send(x_ref, xall.at[t], x_send.at[len(chips)], x_recv.at[t], {"tp": partner})
    xall[pl.ds(t, 1)] = x_ref[...][None]

    first_half = lax.broadcasted_iota(jnp.int32, (length, 2 * WIDTH), 0) < HALF
    centre = [run[HALF // 2 - 1 : HALF // 2], run[HALF + HALF // 2 - 1 : HALF + HALF // 2]]
    middle = jnp.where(first_half, centre[0], centre[1])
    grow = jnp.exp(run - middle)
    shrink = jnp.exp(middle - run)
    from_start = jnp.exp(run)
    keys = pair_of(key * shrink)
    step_f = jnp.exp(centre[1][:, :WIDTH] - centre[0][:, :WIDTH])
    step_b = jnp.exp(centre[0][:, WIDTH:] - centre[1][:, WIDTH:])

    for o in range(1, ny):
        k = at_y(o)
        arrived(dec_y.at[k], dy_send.at[o], dy_recv.at[k], {"sp_1": k})
    decays1 = [dec_y[k] for k in range(ny)]
    line_total = sum(decays1[1:], decays1[0])
    dec_z[pl.ds(z, 1)] = line_total[None]
    for o in far_first(nz):
        k = at_z(o)
        send(dec_z.at[z], dec_z.at[z], dz_send.at[o], dz_recv.at[z], {"sp_0": k})
    first_wait(in1, a1s, a1r)
    up, down, total_up, total_down = line_fold(in1, decays1)
    second_phase(mid1, got1, (total_up, total_down), b1s, b1r)

    for i, k in enumerate(chips):
        arrived(xall.at[k], x_send.at[i], x_recv.at[k], {"tp": k})
        send(xall.at[k], xall.at[k], x_send.at[len(chips) + 1 + i], x_recv.at[k], {"tp": partner})

    for o in range(1, nz):
        k = at_z(o)
        arrived(dec_z.at[k], dz_send.at[o], dz_recv.at[k], {"sp_0": k})
    second_wait(got1, b1s, b1r)
    lines1 = [dec_z[k] for k in range(nz)]
    entry = line_entry(got1, lines1)
    third_phase(back1, state1, entry, (up, down), decays1, c1s, c1r)

    for k in [partner] + [k + 1 - 2 * lax.rem(k, 2) for k in chips]:
        arrived(xall.at[k], x_send.at[0], x_recv.at[k], {"tp": partner})
    raw = jnp.zeros((length, WIDTH), F32)
    for k in range(nt):
        raw += dot(xall[k], w_ref[pl.ds(k * width_in, width_in), :], NN)
    raw = raw.astype(BF16).astype(F32)
    sig = jax.nn.sigmoid(raw)
    root = WIDTH**-0.5
    query = both(raw * sig * root)
    queries = query * grow
    query_in = pair_of(query * from_start)

    lo, hi = slice(0, HALF), slice(HALF, 2 * HALF)
    fw, bw = slice(0, WIDTH), slice(WIDTH, 2 * WIDTH)
    far_f = pair_of(queries[hi, fw] * step_f)
    far_b = pair_of(queries[lo, bw] * step_b)
    queries = pair_of(queries)
    low = lower[lo, lo]
    upp = upper[lo, lo]

    def near(a):
        return jnp.where(low, dot(cut(queries, a, fw), cut(keys, a, fw), NT), 0.0) + jnp.where(
            upp, dot(cut(queries, a, bw), cut(keys, a, bw), NT), 0.0
        )

    scores = jnp.concatenate(
        [
            jnp.concatenate([near(lo), dot(far_b, cut(keys, hi, bw), NT)], axis=1),
            jnp.concatenate([dot(far_f, cut(keys, lo, fw), NT), near(hi)], axis=1),
        ],
        axis=0,
    )
    scores = pair_of(scores)
    inside = dot(scores, v, NN)
    for k in range(nt):
        xturn[pl.ds(k * width_in, width_in), :] = xall[k].T

    third_wait(state1, c1s, c1r)
    state = state1[...]
    mixed = inside + dot(query_in, state, NT)
    inv = lax.rsqrt(jnp.mean(mixed * mixed, axis=1, keepdims=True) + EPS)
    weighted = cot_ref[...].astype(F32) * scale_ref[...]
    along = jnp.mean(weighted * mixed, axis=1, keepdims=True)
    grad_out = pair_of(inv * (weighted - mixed * (inv * inv * along)))

    sense = dot(grad_out, query_in, TN)
    out2[...] = swapped(sense).astype(BF16).reshape(ny, rows, 2 * WIDTH)
    in2[pl.ds(y, 1)] = out2[pl.ds(y, 1)]
    first_phase(out2, in2, a2s, a2r)

    cross = dot(grad_out, v, NT)
    cross_low = [pair_of(jnp.where(low, cross[a, a], 0.0)) for a in (lo, hi)]
    cross_upp = [pair_of(jnp.where(upp, cross[a, a], 0.0)) for a in (lo, hi)]
    cross_f, cross_b = pair_of(cross[hi, lo]), pair_of(cross[lo, hi])
    dq_f = jnp.concatenate(
        [
            dot(cross_low[0], cut(keys, lo, fw), NN),
            dot(cross_low[1], cut(keys, hi, fw), NN) + step_f * dot(cross_f, cut(keys, lo, fw), NN),
        ],
        axis=0,
    )
    dq_b = jnp.concatenate(
        [
            dot(cross_upp[0], cut(keys, lo, bw), NN) + step_b * dot(cross_b, cut(keys, hi, bw), NN),
            dot(cross_upp[1], cut(keys, hi, bw), NN),
        ],
        axis=0,
    )
    dq = grow * jnp.concatenate([dq_f, dq_b], axis=1) + from_start * dot(grad_out, state, NN)
    draw = (dq[:, fw] + dq[:, bw]) * (root * sig * (1.0 + raw * (1.0 - sig)))
    draw = draw.astype(BF16)
    dq_ref[...] = draw
    part = wg.shape[1] * wg.shape[2]
    for k in range(nz):
        wg[k] = dot(xturn[pl.ds(k * part, part), :], draw, NN).astype(BF16).reshape(wg.shape[1:])
    for o in far_first(ny):
        k = at_y(o)
        send(wg.at[:, k], wg_in.at[y], ws.at[o], wr.at[y], {"sp_1": k})

    decays2 = [swapped(d) for d in decays1]
    lines2 = [swapped(d) for d in lines1]
    first_wait(in2, a2s, a2r)
    up, down, total_up, total_down = line_fold(in2, decays2)
    second_phase(mid2, got2, (total_up, total_down), b2s, b2r)

    dv = dot(scores, grad_out, TN)
    dk_f = jnp.concatenate(
        [
            dot(cross_low[0], cut(queries, lo, fw), TN) + dot(cross_f, far_f, TN),
            dot(cross_low[1], cut(queries, hi, fw), TN),
        ],
        axis=0,
    )
    dk_b = jnp.concatenate(
        [
            dot(cross_upp[0], cut(queries, lo, bw), TN),
            dot(cross_upp[1], cut(queries, hi, bw), TN) + dot(cross_b, far_b, TN),
        ],
        axis=0,
    )
    dk = shrink * jnp.concatenate([dk_f, dk_b], axis=1)
    drift = query * dq - key * dk
    left = jnp.exp(closing) * state.astype(F32) + local

    second_wait(got2, b2s, b2r)
    entry = line_entry(got2, lines2)
    third_phase(back2, state2, entry, (up, down), decays2, c2s, c2r)

    for o in range(1, ny):
        k = at_y(o)
        arrived(wg_in.at[k], ws.at[o], wr.at[k], {"sp_1": k})
    acc = wg[:, pl.ds(y, 1)].astype(F32).reshape(wg_mid.shape)
    for o in range(1, ny):
        acc += wg_in[pl.ds(at_y(o), 1)].astype(F32).reshape(wg_mid.shape)
    wg_mid[...] = acc.astype(BF16)
    for o in far_first(nz):
        k = at_z(o)
        send(wg_mid.at[k], wg_got.at[z], zs.at[o], zr.at[z], {"sp_0": k})
    wg_got[pl.ds(z, 1)] = wg_mid[pl.ds(z, 1)]

    third_wait(state2, c2s, c2r)
    after = swapped(state2[...])
    dv_ref[...] = (dv + dot(key_end, after, NT)).astype(BF16)
    dk_end = to_end * dot(v, after, NN)
    ends = jnp.sum(after.astype(F32) * left, axis=0, keepdims=True)
    drift = drift - key * dk_end
    drift = jnp.concatenate(
        [summed(upper_ones, drift[:, fw], 2), summed(lower_ones, drift[:, bw], 2)], axis=1
    )
    dkey = dk + dk_end - (drift + ends) / (1.0 - key)
    dgate = -key * (1.0 - gate) * dkey
    dgf_ref[...] = dgate[:, fw]
    dgb_ref[...] = dgate[:, bw]

    for o in range(1, nz):
        k = at_z(o)
        arrived(wg_got.at[k], zs.at[o], zr.at[k], {"sp_0": k})
    total = wg_got[0].astype(F32)
    for k in range(1, nz):
        total += wg_got[k].astype(F32)
    dw_ref[...] = total

    for copy in sent:
        copy.wait_send()


def on_device(nz, ny, x, w, v, gf, gb, slack, extra, scale, cot):
    nt = w.shape[0] // x.shape[1]
    length = v.shape[0]
    rows = WIDTH // ny
    depth = w.shape[0] // (nz * ny)
    lanes = 2 * WIDTH
    dma = pltpu.SemaphoreType.DMA

    def scan_buffers():
        return [
            pltpu.VMEM((ny, rows, lanes), BF16),
            pltpu.VMEM((ny, rows, lanes), BF16),
            pltpu.VMEM((2, rows, WIDTH), BF16),
            pltpu.VMEM((nz, rows, WIDTH), BF16),
            pltpu.VMEM((ny, rows, lanes), BF16),
            pltpu.VMEM((WIDTH, lanes), BF16),
        ]

    vmem = pl.BlockSpec(memory_space=pltpu.VMEM)
    return pl.pallas_call(
        functools.partial(kernel, nz, ny, nt),
        out_shape=(
            jax.ShapeDtypeStruct((length, WIDTH), BF16),
            jax.ShapeDtypeStruct((length, WIDTH), F32),
            jax.ShapeDtypeStruct((length, WIDTH), F32),
            jax.ShapeDtypeStruct((length, WIDTH), BF16),
            jax.ShapeDtypeStruct((depth, WIDTH), F32),
        ),
        in_specs=[vmem] * 9,
        out_specs=[vmem] * 5,
        scratch_shapes=[
            pltpu.VMEM((nt, length, x.shape[1]), BF16),
            pltpu.VMEM((w.shape[0], length), BF16),
            pltpu.VMEM((ny, 1, lanes), F32),
            pltpu.VMEM((nz, 1, lanes), F32),
            pltpu.VMEM((8, lanes), F32),
        ]
        + scan_buffers()
        + scan_buffers()
        + [
            pltpu.VMEM((nz, ny, depth, WIDTH), BF16),
            pltpu.VMEM((ny, nz, depth, WIDTH), BF16),
            pltpu.VMEM((nz, depth, WIDTH), BF16),
            pltpu.VMEM((nz, depth, WIDTH), BF16),
            dma((nt,)), dma((nt,)), dma((ny,)), dma((ny,)), dma((nz,)), dma((nz,)),
        ]
        + [dma((n,)) for n in (ny, ny, nz, nz, ny, ny)] * 2
        + [dma((n,)) for n in (ny, ny, nz, nz)],
        compiler_params=pltpu.CompilerParams(collective_id=0, has_side_effects=True),
    )(x, w, v, gf, gb, slack, extra.transpose(0, 2, 1), scale.reshape(1, WIDTH), cot)


def solution(mesh):
    torus = Mesh(mesh.devices.reshape(NZ, NY, mesh.shape["tp"]), ("sp_0", "sp_1", "tp"))
    sp = ("sp_0", "sp_1")
    return jax.shard_map(
        functools.partial(on_device, NZ, NY),
        mesh=torus,
        in_specs=(
            P(sp, "tp"),
            P(None, "tp"),
            P(sp, "tp"),
            P(sp, "tp"),
            P(sp, "tp"),
            P(None, "tp"),
            P(None, sp, "tp"),
            P("tp"),
            P(sp, "tp"),
        ),
        out_specs=(P(sp, "tp"),) * 5,
        check_vma=False,
    )
```

```python
import functools

import jax
import jax.numpy as jnp
from jax import lax
from jax.experimental import pallas as pl
from jax.experimental.pallas import tpu as pltpu
from jax.sharding import Mesh
from jax.sharding import PartitionSpec as P

WIDTH = 128
HALF = 128
NZ, NY = 12, 8
NEAR = 3
EPS = 1e-6
MESH_ID = pl.DeviceIdType.MESH
F32, BF16 = jnp.float32, jnp.bfloat16

NN = (((1,), (0,)), ((), ()))
NT = (((1,), (1,)), ((), ()))
TN = (((0,), (0,)), ((), ()))


def dot(a, b, dims):
    a, b = (p if isinstance(p, tuple) else (p,) for p in (a, b))
    total = lax.dot_general(a[0], b[0], dims, preferred_element_type=F32)
    for tail in a[1:]:
        total += lax.dot_general(tail, b[0], dims, preferred_element_type=F32)
    for tail in b[1:]:
        total += lax.dot_general(a[0], tail, dims, preferred_element_type=F32)
    return total


def pair_of(x):
    head = x.astype(BF16)
    return head, (x - head.astype(F32)).astype(BF16)


def cut(pair, *at):
    return tuple(part[at] for part in pair)


def pieces(x, count):
    parts = []
    for _ in range(count):
        part = x.astype(BF16)
        parts.append(part)
        x = x - part.astype(F32)
    return parts


def summed(triangle, x, count):
    return sum(dot(triangle, part, NN) for part in pieces(x, count))


def both(x):
    return jnp.concatenate([x, x], axis=1)


def swapped(x):
    return jnp.concatenate([x[:, WIDTH:], x[:, :WIDTH]], axis=1)


def remote(src, dst, send, recv, peer):
    return pltpu.make_async_remote_copy(
        src_ref=src, dst_ref=dst, send_sem=send, recv_sem=recv, device_id=peer, device_id_type=MESH_ID
    )


def kernel(
    nz, ny, nt,
    x_hbm, w_hbm, v_hbm, gf_hbm, gb_hbm, slack_hbm, extra_hbm, scale_hbm, cot_hbm,
    dq_ref, dgf_ref, dgb_ref, dv_ref, dw_ref,
    w_ref, v_ref, gf_ref, gb_ref, slack_ref, extra_ref, scale_ref, cot_ref, load_sem,
    xall, xturn, dec_y, dec_z,
    out1, in1, mid1, got1, back1, state1,
    out2, in2, mid2, got2, back2, state2,
    wa, wa_in, wa_mid, wa_got, wb, wb_in, wb_mid, wb_got,
    x_send, x_recv, dy_send, dy_recv, dz_send, dz_recv,
    a1s, a1r, b1s, b1r, c1s, c1r,
    a2s, a2r, b2s, b2r, c2s, c2r,
    a3s, a3r, b3s, b3r, a4s, a4r, b4s, b4r,
):
    z, y, t = lax.axis_index("sp_0"), lax.axis_index("sp_1"), lax.axis_index("tp")
    rows = WIDTH // ny
    length = v_ref.shape[0]
    width_in = xall.shape[2]

    def far_first(n):
        return sorted(range(1, n), key=lambda o: -min(o, n - o))

    def at_y(o):
        return lax.rem(y + o, ny)

    def at_z(o):
        return lax.rem(z + o, nz)

    partner = t + 1 - 2 * lax.rem(t, 2)
    chips = [lax.rem(t + 2 * o, nt) for o in far_first(nt // 2)]

    barrier = pltpu.get_barrier_semaphore()
    count = 0
    for o in range(1, nz):
        pl.semaphore_signal(barrier, inc=1, device_id={"sp_0": at_z(o)}, device_id_type=MESH_ID)
        count += 1
    for o in range(1, ny):
        pl.semaphore_signal(barrier, inc=1, device_id={"sp_1": at_y(o)}, device_id_type=MESH_ID)
        count += 1
    for k in [partner] + chips:
        pl.semaphore_signal(barrier, inc=1, device_id={"tp": k}, device_id_type=MESH_ID)
        count += 1

    loads = []
    for i, (src, dst) in enumerate(
        (
            (gf_hbm, gf_ref),
            (gb_hbm, gb_ref),
            (slack_hbm, slack_ref),
            (extra_hbm, extra_ref),
            (v_hbm, v_ref),
            (x_hbm, xall.at[t]),
            (w_hbm, w_ref),
            (cot_hbm, cot_ref),
            (scale_hbm, scale_ref),
        )
    ):
        load = pltpu.make_async_copy(src, dst, load_sem.at[i])
        load.start()
        loads.append(load)

    sent = []

    def send(src, dst, send_sem, recv_sem, peer):
        copy = remote(src, dst, send_sem, recv_sem, peer)
        copy.start()
        sent.append(copy)

    def arrived(dst, send_sem, recv_sem, peer):
        remote(dst, dst, send_sem, recv_sem, peer).wait_recv()

    for load in loads[:4]:
        load.wait()
    pre = jnp.concatenate([gf_ref[...], gb_ref[...]], axis=1).astype(F32)
    slack = jnp.concatenate([slack_ref[0:1, :], slack_ref[1:2, :]], axis=1)
    gate = jax.nn.sigmoid(-pre)
    key = slack * gate
    forget = jnp.log1p(-key)
    row_id = lax.broadcasted_iota(jnp.int32, (length, length), 0)
    col_id = lax.broadcasted_iota(jnp.int32, (length, length), 1)
    lower = row_id >= col_id
    upper = row_id <= col_id
    lower_ones = jnp.where(lower, 1.0, 0.0).astype(BF16)
    upper_ones = jnp.where(upper, 1.0, 0.0).astype(BF16)
    spikes_f = jnp.sum(jnp.where(lower, extra_ref[0], 0.0), axis=1, keepdims=True)
    spikes_b = jnp.sum(jnp.where(upper, extra_ref[1], 0.0), axis=1, keepdims=True)
    run = jnp.concatenate(
        [
            summed(lower_ones, forget[:, :WIDTH], 3) + spikes_f,
            summed(upper_ones, forget[:, WIDTH:], 3) + spikes_b,
        ],
        axis=1,
    )
    closing = jnp.concatenate([run[length - 1 :, :WIDTH], run[0:1, WIDTH:]], axis=1)
    to_end = jnp.exp(closing - run)
    key_end = (key * to_end).astype(BF16)
    loads[4].wait()
    v = v_ref[...]
    local = dot(v, key_end, TN)
    out1[...] = local.astype(BF16).reshape(ny, rows, 2 * WIDTH)
    dec_y[pl.ds(y, 1)] = closing[None]
    in1[pl.ds(y, 1)] = out1[pl.ds(y, 1)]

    pl.semaphore_wait(barrier, count)

    def first_phase(out, into, ss, rs):
        for o in far_first(ny):
            k = at_y(o)
            send(out.at[k], into.at[y], ss.at[o], rs.at[y], {"sp_1": k})

    def first_wait(into, ss, rs):
        for o in range(1, ny):
            k = at_y(o)
            arrived(into.at[k], ss.at[o], rs.at[k], {"sp_1": k})

    def line_fold(into, decays):
        up, down = [None] * ny, [None] * ny
        total = jnp.zeros((rows, WIDTH), F32)
        for k in range(ny):
            up[k] = total
            total = jnp.exp(decays[k][:, :WIDTH]) * total + into[k, :, :WIDTH].astype(F32)
        total_up = total
        total = jnp.zeros((rows, WIDTH), F32)
        for k in reversed(range(ny)):
            down[k] = total
            total = jnp.exp(decays[k][:, WIDTH:]) * total + into[k, :, WIDTH:].astype(F32)
        return up, down, total_up, total

    def second_phase(mid, got, totals, ss, rs):
        mid[0] = totals[0].astype(BF16)
        mid[1] = totals[1].astype(BF16)
        got[pl.ds(z, 1)] = jnp.zeros((1, rows, WIDTH), BF16)
        for o in far_first(nz):
            k = at_z(o)
            side = jnp.where(k > z, 0, 1)
            send(mid.at[side], got.at[z], ss.at[o], rs.at[z], {"sp_0": k})

    def second_wait(got, ss, rs):
        for o in range(1, nz):
            k = at_z(o)
            arrived(got.at[k], ss.at[o], rs.at[k], {"sp_0": k})

    def line_entry(got, decays):
        above = jnp.zeros((rows, WIDTH), F32)
        for k in range(nz):
            new = jnp.exp(decays[k][:, :WIDTH]) * above + got[k].astype(F32)
            above = jnp.where(k < z, new, above)
        below = jnp.zeros((rows, WIDTH), F32)
        for k in reversed(range(nz)):
            new = jnp.exp(decays[k][:, WIDTH:]) * below + got[k].astype(F32)
            below = jnp.where(k > z, new, below)
        return above, below

    def third_phase(back, state, entry, prefixes, decays, ss, rs):
        above, below = entry
        up, down = prefixes
        gone = jnp.zeros((1, WIDTH), F32)
        first = []
        for k in range(ny):
            first.append(jnp.exp(gone) * above + up[k])
            gone = gone + decays[k][:, :WIDTH]
        gone = jnp.zeros((1, WIDTH), F32)
        second = [None] * ny
        for k in reversed(range(ny)):
            second[k] = jnp.exp(gone) * below + down[k]
            gone = gone + decays[k][:, WIDTH:]
        for k in range(ny):
            back[k] = jnp.concatenate([first[k], second[k]], axis=1).astype(BF16)
        here = pl.ds(pl.multiple_of(y * rows, rows), rows)
        for o in far_first(ny):
            k = at_y(o)
            send(back.at[k], state.at[here, :], ss.at[o], rs.at[y], {"sp_1": k})
        state[here, :] = back[pl.ds(y, 1)].reshape(rows, 2 * WIDTH)

    def third_wait(state, ss, rs):
        for o in range(1, ny):
            k = at_y(o)
            there = pl.ds(pl.multiple_of(k * rows, rows), rows)
            arrived(state.at[there, :], ss.at[o], rs.at[k], {"sp_1": k})

    for o in far_first(ny):
        k = at_y(o)
        send(dec_y.at[y], dec_y.at[y], dy_send.at[o], dy_recv.at[y], {"sp_1": k})
    first_phase(out1, in1, a1s, a1r)
    loads[5].wait()
    for i, k in enumerate(chips):
        send(xall.at[t], xall.at[t], x_send.at[i], x_recv.at[t], {"tp": k})
    send(xall.at[t], xall.at[t], x_send.at[len(chips)], x_recv.at[t], {"tp": partner})

    first_half = lax.broadcasted_iota(jnp.int32, (length, 2 * WIDTH), 0) < HALF
    centre = [run[HALF // 2 - 1 : HALF // 2], run[HALF + HALF // 2 - 1 : HALF + HALF // 2]]
    middle = jnp.where(first_half, centre[0], centre[1])
    grow = jnp.exp(run - middle)
    shrink = jnp.exp(middle - run)
    from_start = jnp.exp(run)
    keys = pair_of(key * shrink)
    step_f = jnp.exp(centre[1][:, :WIDTH] - centre[0][:, :WIDTH])
    step_b = jnp.exp(centre[0][:, WIDTH:] - centre[1][:, WIDTH:])

    for o in range(1, ny):
        k = at_y(o)
        arrived(dec_y.at[k], dy_send.at[o], dy_recv.at[k], {"sp_1": k})
    decays1 = [dec_y[k] for k in range(ny)]
    line_total = sum(decays1[1:], decays1[0])
    dec_z[pl.ds(z, 1)] = line_total[None]
    for o in far_first(nz):
        k = at_z(o)
        send(dec_z.at[z], dec_z.at[z], dz_send.at[o], dz_recv.at[z], {"sp_0": k})
    first_wait(in1, a1s, a1r)
    up, down, total_up, total_down = line_fold(in1, decays1)
    second_phase(mid1, got1, (total_up, total_down), b1s, b1r)

    for o in range(1, nz):
        k = at_z(o)
        arrived(dec_z.at[k], dz_send.at[o], dz_recv.at[k], {"sp_0": k})
    second_wait(got1, b1s, b1r)
    lines1 = [dec_z[k] for k in range(nz)]
    entry = line_entry(got1, lines1)
    third_phase(back1, state1, entry, (up, down), decays1, c1s, c1r)

    for i, k in enumerate(chips):
        arrived(xall.at[k], x_send.at[i], x_recv.at[k], {"tp": k})
        send(xall.at[k], xall.at[k], x_send.at[len(chips) + 1 + i], x_recv.at[k], {"tp": partner})

    for k in [partner] + [k + 1 - 2 * lax.rem(k, 2) for k in chips]:
        arrived(xall.at[k], x_send.at[0], x_recv.at[k], {"tp": partner})
    for load in loads[6:]:
        load.wait()
    raw = jnp.zeros((length, WIDTH), F32)
    for k in range(nt):
        raw += dot(xall[k], w_ref[pl.ds(k * width_in, width_in), :], NN)
    raw = raw.astype(BF16).astype(F32)
    sig = jax.nn.sigmoid(raw)
    root = WIDTH**-0.5
    query = both(raw * sig * root)
    queries = query * grow
    query_in = pair_of(query * from_start)

    lo, hi = slice(0, HALF), slice(HALF, 2 * HALF)
    fw, bw = slice(0, WIDTH), slice(WIDTH, 2 * WIDTH)
    far_f = pair_of(queries[hi, fw] * step_f)
    far_b = pair_of(queries[lo, bw] * step_b)
    queries = pair_of(queries)
    low = lower[lo, lo]
    upp = upper[lo, lo]

    def near(a):
        return jnp.where(low, dot(cut(queries, a, fw), cut(keys, a, fw), NT), 0.0) + jnp.where(
            upp, dot(cut(queries, a, bw), cut(keys, a, bw), NT), 0.0
        )

    scores = jnp.concatenate(
        [
            jnp.concatenate([near(lo), dot(far_b, cut(keys, hi, bw), NT)], axis=1),
            jnp.concatenate([dot(far_f, cut(keys, lo, fw), NT), near(hi)], axis=1),
        ],
        axis=0,
    )
    scores = pair_of(scores)
    inside = dot(scores, v, NN)
    for k in range(nt):
        xturn[pl.ds(k * width_in, width_in), :] = xall[k].T

    third_wait(state1, c1s, c1r)
    state = state1[...]
    mixed = inside + dot(query_in, state, NT)
    inv = lax.rsqrt(jnp.mean(mixed * mixed, axis=1, keepdims=True) + EPS)
    weighted = cot_ref[...].astype(F32) * scale_ref[...]
    along = jnp.mean(weighted * mixed, axis=1, keepdims=True)
    grad_out = pair_of(inv * (weighted - mixed * (inv * inv * along)))

    sense = dot(grad_out, query_in, TN)
    out2[...] = swapped(sense).astype(BF16).reshape(ny, rows, 2 * WIDTH)
    in2[pl.ds(y, 1)] = out2[pl.ds(y, 1)]
    first_phase(out2, in2, a2s, a2r)

    cross = dot(grad_out, v, NT)
    cross_low = [pair_of(jnp.where(low, cross[a, a], 0.0)) for a in (lo, hi)]
    cross_upp = [pair_of(jnp.where(upp, cross[a, a], 0.0)) for a in (lo, hi)]
    cross_f, cross_b = pair_of(cross[hi, lo]), pair_of(cross[lo, hi])
    dq_f = jnp.concatenate(
        [
            dot(cross_low[0], cut(keys, lo, fw), NN),
            dot(cross_low[1], cut(keys, hi, fw), NN) + step_f * dot(cross_f, cut(keys, lo, fw), NN),
        ],
        axis=0,
    )
    dq_b = jnp.concatenate(
        [
            dot(cross_upp[0], cut(keys, lo, bw), NN) + step_b * dot(cross_b, cut(keys, hi, bw), NN),
            dot(cross_upp[1], cut(keys, hi, bw), NN),
        ],
        axis=0,
    )
    dq = grow * jnp.concatenate([dq_f, dq_b], axis=1) + from_start * dot(grad_out, state, NN)
    draw = (dq[:, fw] + dq[:, bw]) * (root * sig * (1.0 + raw * (1.0 - sig)))
    draw = draw.astype(BF16)
    dq_ref[...] = draw

    part = ny * wa.shape[2]

    def terms(o):
        owner = pl.multiple_of(at_z(o) * part, part)
        return dot(xturn[pl.ds(owner, part), :], draw, NN).astype(BF16).reshape(wa.shape[1:])

    near_z = [o for o in range(1, nz) if min(o, nz - o) <= NEAR]
    far_z = [o for o in range(nz) if o not in near_z]
    for i, o in enumerate(far_z):
        wa[i] = terms(o)
    for o in far_first(ny):
        k = at_y(o)
        send(wa.at[:, k], wa_in.at[y], a3s.at[o], a3r.at[y], {"sp_1": k})
    for i, o in enumerate(near_z):
        wb[i] = terms(o)

    decays2 = [swapped(d) for d in decays1]
    lines2 = [swapped(d) for d in lines1]
    first_wait(in2, a2s, a2r)
    up, down, total_up, total_down = line_fold(in2, decays2)
    second_phase(mid2, got2, (total_up, total_down), b2s, b2r)
    for i in sorted(range(len(near_z)), key=lambda i: -min(near_z[i], nz - near_z[i])):
        send(wb.at[i], wb_in.at[i], b3s.at[i], b3r.at[i], {"sp_0": at_z(near_z[i])})

    dv = dot(scores, grad_out, TN)
    dk_f = jnp.concatenate(
        [
            dot(cross_low[0], cut(queries, lo, fw), TN) + dot(cross_f, far_f, TN),
            dot(cross_low[1], cut(queries, hi, fw), TN),
        ],
        axis=0,
    )
    dk_b = jnp.concatenate(
        [
            dot(cross_upp[0], cut(queries, lo, bw), TN),
            dot(cross_upp[1], cut(queries, hi, bw), TN) + dot(cross_b, far_b, TN),
        ],
        axis=0,
    )
    dk = shrink * jnp.concatenate([dk_f, dk_b], axis=1)
    drift = query * dq - key * dk
    left = jnp.exp(closing) * state.astype(F32) + local

    second_wait(got2, b2s, b2r)
    entry = line_entry(got2, lines2)
    third_phase(back2, state2, entry, (up, down), decays2, c2s, c2r)

    for o in range(1, ny):
        k = at_y(o)
        arrived(wa_in.at[k], a3s.at[o], a3r.at[k], {"sp_1": k})
    acc = wa[:, pl.ds(y, 1)].astype(F32).reshape(wa_mid.shape)
    for o in range(1, ny):
        acc += wa_in[pl.ds(at_y(o), 1)].astype(F32).reshape(wa_mid.shape)
    own = acc[0]
    wa_mid[...] = acc.astype(BF16)
    for i in sorted(range(1, len(far_z)), key=lambda i: -min(far_z[i], nz - far_z[i])):
        send(wa_mid.at[i], wa_got.at[i], b4s.at[i], b4r.at[i], {"sp_0": at_z(far_z[i])})

    for i, o in enumerate(near_z):
        arrived(wb_in.at[i], b3s.at[i], b3r.at[i], {"sp_0": at_z(nz - o)})
    acc = wb_in[0].astype(F32)
    for i in range(1, len(near_z)):
        acc += wb_in[i].astype(F32)
    wb_mid[...] = acc.astype(BF16)
    for o in far_first(ny):
        k = at_y(o)
        send(wb_mid.at[k], wb_got.at[y], a4s.at[o], a4r.at[y], {"sp_1": k})
    own += wb_mid[pl.ds(y, 1)].astype(F32).reshape(own.shape)

    third_wait(state2, c2s, c2r)
    after = swapped(state2[...])
    dv_ref[...] = (dv + dot(key_end, after, NT)).astype(BF16)
    dk_end = to_end * dot(v, after, NN)
    ends = jnp.sum(after.astype(F32) * left, axis=0, keepdims=True)
    drift = drift - key * dk_end
    drift = jnp.concatenate(
        [summed(upper_ones, drift[:, fw], 2), summed(lower_ones, drift[:, bw], 2)], axis=1
    )
    dkey = dk + dk_end - (drift + ends) / (1.0 - key)
    dgate = -key * (1.0 - gate) * dkey
    dgf_ref[...] = dgate[:, fw]
    dgb_ref[...] = dgate[:, bw]

    for i in range(1, len(far_z)):
        arrived(wa_got.at[i], b4s.at[i], b4r.at[i], {"sp_0": at_z(nz - far_z[i])})
        own += wa_got[i].astype(F32)
    for o in range(1, ny):
        k = at_y(o)
        arrived(wb_got.at[k], a4s.at[o], a4r.at[k], {"sp_1": k})
        own += wb_got[pl.ds(k, 1)].astype(F32).reshape(own.shape)
    dw_ref[...] = own

    for copy in sent:
        copy.wait_send()


def store(*refs):
    sources, targets, sems = refs[:5], refs[5:10], refs[10]
    copies = [
        pltpu.make_async_copy(src, dst, sems.at[i])
        for i, (src, dst) in enumerate(zip(sources, targets))
    ]
    for copy in copies:
        copy.start()
    for copy in copies:
        copy.wait()


def in_vmem(a):
    return pltpu.with_memory_space_constraint(a, pltpu.VMEM)


def on_device(nz, ny, x, w, v, gf, gb, slack, extra, scale, cot):
    nt = w.shape[0] // x.shape[1]
    length = v.shape[0]
    rows = WIDTH // ny
    depth = w.shape[0] // (nz * ny)
    lanes = 2 * WIDTH
    dma = pltpu.SemaphoreType.DMA

    def scan_buffers():
        return [
            pltpu.VMEM((ny, rows, lanes), BF16),
            pltpu.VMEM((ny, rows, lanes), BF16),
            pltpu.VMEM((2, rows, WIDTH), BF16),
            pltpu.VMEM((nz, rows, WIDTH), BF16),
            pltpu.VMEM((ny, rows, lanes), BF16),
            pltpu.VMEM((WIDTH, lanes), BF16),
        ]

    results = (
        ((length, WIDTH), BF16),
        ((length, WIDTH), F32),
        ((length, WIDTH), F32),
        ((length, WIDTH), BF16),
        ((depth, WIDTH), F32),
    )
    near = sum(1 for o in range(1, nz) if min(o, nz - o) <= NEAR)
    far = nz - near
    vmem = pl.BlockSpec(memory_space=pltpu.VMEM)
    anywhere = pl.BlockSpec(memory_space=pl.ANY)
    held = pl.pallas_call(
        functools.partial(kernel, nz, ny, nt),
        out_shape=tuple(pltpu.VMEM(shape, dtype) for shape, dtype in results),
        in_specs=[anywhere] * 9,
        out_specs=[vmem] * 5,
        scratch_shapes=[
            pltpu.VMEM(w.shape, BF16),
            pltpu.VMEM(v.shape, BF16),
            pltpu.VMEM(gf.shape, BF16),
            pltpu.VMEM(gb.shape, BF16),
            pltpu.VMEM(slack.shape, F32),
            pltpu.VMEM((2, 1, length), F32),
            pltpu.VMEM((1, WIDTH), F32),
            pltpu.VMEM(cot.shape, BF16),
            dma((9,)),
            pltpu.VMEM((nt, length, x.shape[1]), BF16),
            pltpu.VMEM((w.shape[0], length), BF16),
            pltpu.VMEM((ny, 1, lanes), F32),
            pltpu.VMEM((nz, 1, lanes), F32),
        ]
        + scan_buffers()
        + scan_buffers()
        + [
            pltpu.VMEM((far, ny, depth, WIDTH), BF16),
            pltpu.VMEM((ny, far, depth, WIDTH), BF16),
            pltpu.VMEM((far, depth, WIDTH), BF16),
            pltpu.VMEM((far, depth, WIDTH), BF16),
            pltpu.VMEM((near, ny, depth, WIDTH), BF16),
            pltpu.VMEM((near, ny, depth, WIDTH), BF16),
            pltpu.VMEM((ny, depth, WIDTH), BF16),
            pltpu.VMEM((ny, depth, WIDTH), BF16),
            dma((nt,)), dma((nt,)), dma((ny,)), dma((ny,)), dma((nz,)), dma((nz,)),
        ]
        + [dma((n,)) for n in (ny, ny, nz, nz, ny, ny)] * 2
        + [dma((n,)) for n in (ny, ny, near, near, ny, ny, far, far)],
        compiler_params=pltpu.CompilerParams(collective_id=0, has_side_effects=True),
    )(x, w, v, gf, gb, slack, extra.transpose(0, 2, 1), scale.reshape(1, WIDTH), cot)
    return pl.pallas_call(
        store,
        out_shape=tuple(jax.ShapeDtypeStruct(shape, dtype) for shape, dtype in results),
        in_specs=[vmem] * 5,
        out_specs=[anywhere] * 5,
        scratch_shapes=[dma((5,))],
    )(*(in_vmem(a) for a in held))


def solution(mesh):
    torus = Mesh(mesh.devices.reshape(NZ, NY, mesh.shape["tp"]), ("sp_0", "sp_1", "tp"))
    sp = ("sp_0", "sp_1")
    return jax.shard_map(
        functools.partial(on_device, NZ, NY),
        mesh=torus,
        in_specs=(
            P(sp, "tp"),
            P(None, "tp"),
            P(sp, "tp"),
            P(sp, "tp"),
            P(sp, "tp"),
            P(None, "tp"),
            P(None, sp, "tp"),
            P("tp"),
            P(sp, "tp"),
        ),
        out_specs=(P(sp, "tp"),) * 5,
        check_vma=False,
    )
```

```python
import functools

import jax
import jax.numpy as jnp
from jax import lax
from jax.experimental import pallas as pl
from jax.experimental.pallas import tpu as pltpu
from jax.sharding import Mesh
from jax.sharding import PartitionSpec as P

WIDTH = 128
HALF = 128
NZ, NY = 12, 8
NEAR = 2
GROUPS = (2, 2)
EPS = 1e-6
MESH_ID = pl.DeviceIdType.MESH
F32, BF16 = jnp.float32, jnp.bfloat16

NN = (((1,), (0,)), ((), ()))
NT = (((1,), (1,)), ((), ()))
TN = (((0,), (0,)), ((), ()))


def dot(a, b, dims):
    a, b = (p if isinstance(p, tuple) else (p,) for p in (a, b))
    total = lax.dot_general(a[0], b[0], dims, preferred_element_type=F32)
    for tail in a[1:]:
        total += lax.dot_general(tail, b[0], dims, preferred_element_type=F32)
    for tail in b[1:]:
        total += lax.dot_general(a[0], tail, dims, preferred_element_type=F32)
    return total


def pair_of(x):
    head = x.astype(BF16)
    return head, (x - head.astype(F32)).astype(BF16)


def cut(pair, *at):
    return tuple(part[at] for part in pair)


def pieces(x, count):
    parts = []
    for _ in range(count):
        part = x.astype(BF16)
        parts.append(part)
        x = x - part.astype(F32)
    return parts


def summed(triangle, x, count):
    return sum(dot(triangle, part, NN) for part in pieces(x, count))


def both(x):
    return jnp.concatenate([x, x], axis=1)


def swapped(x):
    return jnp.concatenate([x[:, WIDTH:], x[:, :WIDTH]], axis=1)


def remote(src, dst, send, recv, peer):
    return pltpu.make_async_remote_copy(
        src_ref=src, dst_ref=dst, send_sem=send, recv_sem=recv, device_id=peer, device_id_type=MESH_ID
    )


def kernel(
    nz, ny, nt,
    x_hbm, w_hbm, v_hbm, gf_hbm, gb_hbm, slack_hbm, extra_hbm, scale_hbm, cot_hbm,
    dq_ref, dgf_ref, dgb_ref, dv_ref, dw_ref,
    w_ref, v_ref, gf_ref, gb_ref, slack_ref, extra_ref, scale_ref, cot_ref, load_sem,
    xall, xturn, dec_y, dec_z,
    out1, in1, mid1, got1, back1, state1,
    out2, in2, mid2, got2, back2, state2,
    wa, wa_in, wa_mid, wa_got, wb, wb_in, wb_mid, wb_got,
    x_send, x_recv, dy_send, dy_recv, dz_send, dz_recv,
    a1s, a1r, b1s, b1r, c1s, c1r,
    a2s, a2r, b2s, b2r, c2s, c2r,
    a3s, a3r, b3s, b3r, a4s, a4r, b4s, b4r,
):
    z, y, t = lax.axis_index("sp_0"), lax.axis_index("sp_1"), lax.axis_index("tp")
    rows = WIDTH // ny
    length = v_ref.shape[0]
    width_in = xall.shape[2]

    def far_first(n):
        return sorted(range(1, n), key=lambda o: -min(o, n - o))

    def at_y(o):
        return lax.rem(y + o, ny)

    def at_z(o):
        return lax.rem(z + o, nz)

    partner = t + 1 - 2 * lax.rem(t, 2)
    chips = [lax.rem(t + 2 * o, nt) for o in far_first(nt // 2)]

    barrier = pltpu.get_barrier_semaphore()
    count = 0
    for o in range(1, nz):
        pl.semaphore_signal(barrier, inc=1, device_id={"sp_0": at_z(o)}, device_id_type=MESH_ID)
        count += 1
    for o in range(1, ny):
        pl.semaphore_signal(barrier, inc=1, device_id={"sp_1": at_y(o)}, device_id_type=MESH_ID)
        count += 1
    for k in [partner] + chips:
        pl.semaphore_signal(barrier, inc=1, device_id={"tp": k}, device_id_type=MESH_ID)
        count += 1

    loads = []
    for i, (src, dst) in enumerate(
        (
            (gf_hbm, gf_ref),
            (gb_hbm, gb_ref),
            (slack_hbm, slack_ref),
            (extra_hbm, extra_ref),
            (v_hbm, v_ref),
            (x_hbm, xall.at[t]),
            (w_hbm, w_ref),
            (cot_hbm, cot_ref),
            (scale_hbm, scale_ref),
        )
    ):
        load = pltpu.make_async_copy(src, dst, load_sem.at[i])
        load.start()
        loads.append(load)

    sent = []

    def send(src, dst, send_sem, recv_sem, peer):
        copy = remote(src, dst, send_sem, recv_sem, peer)
        copy.start()
        sent.append(copy)

    def arrived(dst, send_sem, recv_sem, peer):
        remote(dst, dst, send_sem, recv_sem, peer).wait_recv()

    for load in loads[:4]:
        load.wait()
    pre = jnp.concatenate([gf_ref[...], gb_ref[...]], axis=1).astype(F32)
    slack = jnp.concatenate([slack_ref[0:1, :], slack_ref[1:2, :]], axis=1)
    gate = jax.nn.sigmoid(-pre)
    key = slack * gate
    forget = jnp.log1p(-key)
    row_id = lax.broadcasted_iota(jnp.int32, (length, length), 0)
    col_id = lax.broadcasted_iota(jnp.int32, (length, length), 1)
    lower = row_id >= col_id
    upper = row_id <= col_id
    lower_ones = jnp.where(lower, 1.0, 0.0).astype(BF16)
    upper_ones = jnp.where(upper, 1.0, 0.0).astype(BF16)
    spikes_f = jnp.sum(jnp.where(lower, extra_ref[0], 0.0), axis=1, keepdims=True)
    spikes_b = jnp.sum(jnp.where(upper, extra_ref[1], 0.0), axis=1, keepdims=True)
    run = jnp.concatenate(
        [
            summed(lower_ones, forget[:, :WIDTH], 3) + spikes_f,
            summed(upper_ones, forget[:, WIDTH:], 3) + spikes_b,
        ],
        axis=1,
    )
    closing = jnp.concatenate([run[length - 1 :, :WIDTH], run[0:1, WIDTH:]], axis=1)
    to_end = jnp.exp(closing - run)
    key_end = (key * to_end).astype(BF16)
    loads[4].wait()
    v = v_ref[...]
    local = dot(v, key_end, TN)
    out1[...] = local.astype(BF16).reshape(ny, rows, 2 * WIDTH)
    dec_y[pl.ds(y, 1)] = closing[None]
    in1[pl.ds(y, 1)] = out1[pl.ds(y, 1)]

    pl.semaphore_wait(barrier, count)

    def first_phase(out, into, ss, rs):
        for o in far_first(ny):
            k = at_y(o)
            send(out.at[k], into.at[y], ss.at[o], rs.at[y], {"sp_1": k})

    def first_wait(into, ss, rs):
        for o in range(1, ny):
            k = at_y(o)
            arrived(into.at[k], ss.at[o], rs.at[k], {"sp_1": k})

    def line_fold(into, decays):
        up, down = [None] * ny, [None] * ny
        total = jnp.zeros((rows, WIDTH), F32)
        for k in range(ny):
            up[k] = total
            total = jnp.exp(decays[k][:, :WIDTH]) * total + into[k, :, :WIDTH].astype(F32)
        total_up = total
        total = jnp.zeros((rows, WIDTH), F32)
        for k in reversed(range(ny)):
            down[k] = total
            total = jnp.exp(decays[k][:, WIDTH:]) * total + into[k, :, WIDTH:].astype(F32)
        return up, down, total_up, total

    def second_phase(mid, got, totals, ss, rs):
        mid[0] = totals[0].astype(BF16)
        mid[1] = totals[1].astype(BF16)
        got[pl.ds(z, 1)] = jnp.zeros((1, rows, WIDTH), BF16)
        for o in far_first(nz):
            k = at_z(o)
            side = jnp.where(k > z, 0, 1)
            send(mid.at[side], got.at[z], ss.at[o], rs.at[z], {"sp_0": k})

    def second_wait(got, ss, rs):
        for o in range(1, nz):
            k = at_z(o)
            arrived(got.at[k], ss.at[o], rs.at[k], {"sp_0": k})

    def line_entry(got, decays):
        above = jnp.zeros((rows, WIDTH), F32)
        for k in range(nz):
            new = jnp.exp(decays[k][:, :WIDTH]) * above + got[k].astype(F32)
            above = jnp.where(k < z, new, above)
        below = jnp.zeros((rows, WIDTH), F32)
        for k in reversed(range(nz)):
            new = jnp.exp(decays[k][:, WIDTH:]) * below + got[k].astype(F32)
            below = jnp.where(k > z, new, below)
        return above, below

    def third_phase(back, state, entry, prefixes, decays, ss, rs):
        above, below = entry
        up, down = prefixes
        gone = jnp.zeros((1, WIDTH), F32)
        first = []
        for k in range(ny):
            first.append(jnp.exp(gone) * above + up[k])
            gone = gone + decays[k][:, :WIDTH]
        gone = jnp.zeros((1, WIDTH), F32)
        second = [None] * ny
        for k in reversed(range(ny)):
            second[k] = jnp.exp(gone) * below + down[k]
            gone = gone + decays[k][:, WIDTH:]
        for k in range(ny):
            back[k] = jnp.concatenate([first[k], second[k]], axis=1).astype(BF16)
        here = pl.ds(pl.multiple_of(y * rows, rows), rows)
        for o in far_first(ny):
            k = at_y(o)
            send(back.at[k], state.at[here, :], ss.at[o], rs.at[y], {"sp_1": k})
        state[here, :] = back[pl.ds(y, 1)].reshape(rows, 2 * WIDTH)

    def third_wait(state, ss, rs):
        for o in range(1, ny):
            k = at_y(o)
            there = pl.ds(pl.multiple_of(k * rows, rows), rows)
            arrived(state.at[there, :], ss.at[o], rs.at[k], {"sp_1": k})

    for o in far_first(ny):
        k = at_y(o)
        send(dec_y.at[y], dec_y.at[y], dy_send.at[o], dy_recv.at[y], {"sp_1": k})
    first_phase(out1, in1, a1s, a1r)
    loads[5].wait()
    for i, k in enumerate(chips):
        send(xall.at[t], xall.at[t], x_send.at[i], x_recv.at[t], {"tp": k})
    send(xall.at[t], xall.at[t], x_send.at[len(chips)], x_recv.at[t], {"tp": partner})

    first_half = lax.broadcasted_iota(jnp.int32, (length, 2 * WIDTH), 0) < HALF
    centre = [run[HALF // 2 - 1 : HALF // 2], run[HALF + HALF // 2 - 1 : HALF + HALF // 2]]
    middle = jnp.where(first_half, centre[0], centre[1])
    grow = jnp.exp(run - middle)
    shrink = jnp.exp(middle - run)
    from_start = jnp.exp(run)
    keys = pair_of(key * shrink)
    step_f = jnp.exp(centre[1][:, :WIDTH] - centre[0][:, :WIDTH])
    step_b = jnp.exp(centre[0][:, WIDTH:] - centre[1][:, WIDTH:])

    for o in range(1, ny):
        k = at_y(o)
        arrived(dec_y.at[k], dy_send.at[o], dy_recv.at[k], {"sp_1": k})
    decays1 = [dec_y[k] for k in range(ny)]
    line_total = sum(decays1[1:], decays1[0])
    dec_z[pl.ds(z, 1)] = line_total[None]
    for o in far_first(nz):
        k = at_z(o)
        send(dec_z.at[z], dec_z.at[z], dz_send.at[o], dz_recv.at[z], {"sp_0": k})
    first_wait(in1, a1s, a1r)
    up, down, total_up, total_down = line_fold(in1, decays1)
    second_phase(mid1, got1, (total_up, total_down), b1s, b1r)

    for o in range(1, nz):
        k = at_z(o)
        arrived(dec_z.at[k], dz_send.at[o], dz_recv.at[k], {"sp_0": k})
    second_wait(got1, b1s, b1r)
    lines1 = [dec_z[k] for k in range(nz)]
    entry = line_entry(got1, lines1)
    third_phase(back1, state1, entry, (up, down), decays1, c1s, c1r)

    for i, k in enumerate(chips):
        arrived(xall.at[k], x_send.at[i], x_recv.at[k], {"tp": k})
        send(xall.at[k], xall.at[k], x_send.at[len(chips) + 1 + i], x_recv.at[k], {"tp": partner})

    for k in [partner] + [k + 1 - 2 * lax.rem(k, 2) for k in chips]:
        arrived(xall.at[k], x_send.at[0], x_recv.at[k], {"tp": partner})
    for load in loads[6:]:
        load.wait()
    raw = jnp.zeros((length, WIDTH), F32)
    for k in range(nt):
        raw += dot(xall[k], w_ref[pl.ds(k * width_in, width_in), :], NN)
    raw = raw.astype(BF16).astype(F32)
    sig = jax.nn.sigmoid(raw)
    root = WIDTH**-0.5
    query = both(raw * sig * root)
    queries = query * grow
    query_in = pair_of(query * from_start)

    lo, hi = slice(0, HALF), slice(HALF, 2 * HALF)
    fw, bw = slice(0, WIDTH), slice(WIDTH, 2 * WIDTH)
    far_f = pair_of(queries[hi, fw] * step_f)
    far_b = pair_of(queries[lo, bw] * step_b)
    queries = pair_of(queries)
    low = lower[lo, lo]
    upp = upper[lo, lo]

    def near(a):
        return jnp.where(low, dot(cut(queries, a, fw), cut(keys, a, fw), NT), 0.0) + jnp.where(
            upp, dot(cut(queries, a, bw), cut(keys, a, bw), NT), 0.0
        )

    scores = jnp.concatenate(
        [
            jnp.concatenate([near(lo), dot(far_b, cut(keys, hi, bw), NT)], axis=1),
            jnp.concatenate([dot(far_f, cut(keys, lo, fw), NT), near(hi)], axis=1),
        ],
        axis=0,
    )
    scores = pair_of(scores)
    inside = dot(scores, v, NN)
    for k in range(nt):
        xturn[pl.ds(k * width_in, width_in), :] = xall[k].T

    third_wait(state1, c1s, c1r)
    state = state1[...]
    mixed = inside + dot(query_in, state, NT)
    inv = lax.rsqrt(jnp.mean(mixed * mixed, axis=1, keepdims=True) + EPS)
    weighted = cot_ref[...].astype(F32) * scale_ref[...]
    along = jnp.mean(weighted * mixed, axis=1, keepdims=True)
    grad_out = pair_of(inv * (weighted - mixed * (inv * inv * along)))

    sense = dot(grad_out, query_in, TN)
    out2[...] = swapped(sense).astype(BF16).reshape(ny, rows, 2 * WIDTH)
    in2[pl.ds(y, 1)] = out2[pl.ds(y, 1)]
    first_phase(out2, in2, a2s, a2r)

    cross = dot(grad_out, v, NT)
    cross_low = [pair_of(jnp.where(low, cross[a, a], 0.0)) for a in (lo, hi)]
    cross_upp = [pair_of(jnp.where(upp, cross[a, a], 0.0)) for a in (lo, hi)]
    cross_f, cross_b = pair_of(cross[hi, lo]), pair_of(cross[lo, hi])
    dq_f = jnp.concatenate(
        [
            dot(cross_low[0], cut(keys, lo, fw), NN),
            dot(cross_low[1], cut(keys, hi, fw), NN) + step_f * dot(cross_f, cut(keys, lo, fw), NN),
        ],
        axis=0,
    )
    dq_b = jnp.concatenate(
        [
            dot(cross_upp[0], cut(keys, lo, bw), NN) + step_b * dot(cross_b, cut(keys, hi, bw), NN),
            dot(cross_upp[1], cut(keys, hi, bw), NN),
        ],
        axis=0,
    )
    dq = grow * jnp.concatenate([dq_f, dq_b], axis=1) + from_start * dot(grad_out, state, NN)
    draw = (dq[:, fw] + dq[:, bw]) * (root * sig * (1.0 + raw * (1.0 - sig)))
    draw = draw.astype(BF16)
    dq_ref[...] = draw

    part = ny * wa.shape[2]
    far, near = nz - 2 * NEAR - 1, 2 * NEAR
    far_turn = sum(jnp.where(z + NEAR + 1 + i < nz, 1, 0) for i in range(far))
    near_at = [i + 1 + (nz - 1 - 2 * NEAR) * (i // NEAR) for i in range(near)]
    near_turn = sum(jnp.where(z + o < nz, 1, 0) for o in near_at)
    first, second = GROUPS
    slots = [*range(first + second), None, *range(first + second, far)]
    groups = [slice(0, first), slice(first, first + second + 1), slice(first + second + 1, far + 1)]

    def far_index(rank):
        return lax.rem(far_turn + rank, far)

    def far_owner(index):
        return lax.rem(z + NEAR + 1 + index, nz)

    def terms(owner):
        start = pl.multiple_of(owner * part, part)
        return dot(xturn[pl.ds(start, part), :], draw, NN).astype(BF16).reshape(wa.shape[1:])

    def far_send(g):
        for o in far_first(ny):
            k = at_y(o)
            send(wa.at[groups[g], k], wa_in.at[y, groups[g]], a3s.at[g, o], a3r.at[g, y], {"sp_1": k})

    def far_pass(g):
        for o in range(1, ny):
            k = at_y(o)
            arrived(wa_in.at[k, groups[g]], a3s.at[g, o], a3r.at[g, k], {"sp_1": k})
        count = groups[g].stop - groups[g].start
        acc = wa[groups[g], pl.ds(y, 1)].astype(F32).reshape(count, *wa_mid.shape[1:])
        for o in range(1, ny):
            acc += wa_in[pl.ds(at_y(o), 1), groups[g]].astype(F32).reshape(acc.shape)
        wa_mid[groups[g]] = acc.astype(BF16)
        kept = None
        for n, rank in enumerate(slots[groups[g]]):
            slot = groups[g].start + n
            if rank is None:
                kept = acc[n]
            else:
                i = far_index(rank)
                send(wa_mid.at[slot], wa_got.at[i], b4s.at[rank], b4r.at[i], {"sp_0": far_owner(i)})
        return kept

    def fill(g):
        for slot in range(groups[g].start, groups[g].stop):
            wa[slot] = terms(z if slots[slot] is None else far_owner(far_index(slots[slot])))

    fill(0)
    far_send(0)
    fill(1)
    far_send(1)
    fill(2)
    far_send(2)
    for i, o in enumerate(near_at):
        wb[i] = terms(at_z(o))

    decays2 = [swapped(d) for d in decays1]
    lines2 = [swapped(d) for d in lines1]
    first_wait(in2, a2s, a2r)
    up, down, total_up, total_down = line_fold(in2, decays2)
    second_phase(mid2, got2, (total_up, total_down), b2s, b2r)
    for rank in range(near):
        i = lax.rem(near_turn + rank, near)
        o = i + 1 + (nz - 1 - 2 * NEAR) * (i // NEAR)
        send(wb.at[i], wb_in.at[i], b3s.at[rank], b3r.at[i], {"sp_0": lax.rem(z + o, nz)})

    dv = dot(scores, grad_out, TN)
    dk_f = jnp.concatenate(
        [
            dot(cross_low[0], cut(queries, lo, fw), TN) + dot(cross_f, far_f, TN),
            dot(cross_low[1], cut(queries, hi, fw), TN),
        ],
        axis=0,
    )
    dk_b = jnp.concatenate(
        [
            dot(cross_upp[0], cut(queries, lo, bw), TN),
            dot(cross_upp[1], cut(queries, hi, bw), TN) + dot(cross_b, far_b, TN),
        ],
        axis=0,
    )
    dk = shrink * jnp.concatenate([dk_f, dk_b], axis=1)
    drift = query * dq - key * dk
    left = jnp.exp(closing) * state.astype(F32) + local

    far_pass(0)
    second_wait(got2, b2s, b2r)
    entry = line_entry(got2, lines2)
    third_phase(back2, state2, entry, (up, down), decays2, c2s, c2r)

    for i, o in enumerate(near_at):
        arrived(wb_in.at[i], b3s.at[i], b3r.at[i], {"sp_0": at_z(nz - o)})
    acc = wb_in[0].astype(F32)
    for i in range(1, near):
        acc += wb_in[i].astype(F32)
    wb_mid[...] = acc.astype(BF16)
    for o in far_first(ny):
        k = at_y(o)
        send(wb_mid.at[k], wb_got.at[y], a4s.at[o], a4r.at[y], {"sp_1": k})
    own = far_pass(1) + wb_mid[pl.ds(y, 1)].astype(F32).reshape(dw_ref.shape)
    far_pass(2)

    third_wait(state2, c2s, c2r)
    after = swapped(state2[...])
    dv_ref[...] = (dv + dot(key_end, after, NT)).astype(BF16)
    dk_end = to_end * dot(v, after, NN)
    ends = jnp.sum(after.astype(F32) * left, axis=0, keepdims=True)
    drift = drift - key * dk_end
    drift = jnp.concatenate(
        [summed(upper_ones, drift[:, fw], 2), summed(lower_ones, drift[:, bw], 2)], axis=1
    )
    dkey = dk + dk_end - (drift + ends) / (1.0 - key)
    dgate = -key * (1.0 - gate) * dkey
    dgf_ref[...] = dgate[:, fw]
    dgb_ref[...] = dgate[:, bw]

    for i in range(far):
        arrived(wa_got.at[i], b4s.at[i], b4r.at[i], {"sp_0": at_z(nz - NEAR - 1 - i)})
        own += wa_got[i].astype(F32)
    for o in range(1, ny):
        k = at_y(o)
        arrived(wb_got.at[k], a4s.at[o], a4r.at[k], {"sp_1": k})
        own += wb_got[pl.ds(k, 1)].astype(F32).reshape(own.shape)
    dw_ref[...] = own

    for copy in sent:
        copy.wait_send()


def store(*refs):
    sources, targets, sems = refs[:5], refs[5:10], refs[10]
    copies = [
        pltpu.make_async_copy(src, dst, sems.at[i])
        for i, (src, dst) in enumerate(zip(sources, targets))
    ]
    for copy in copies:
        copy.start()
    for copy in copies:
        copy.wait()


def in_vmem(a):
    return pltpu.with_memory_space_constraint(a, pltpu.VMEM)


def on_device(nz, ny, x, w, v, gf, gb, slack, extra, scale, cot):
    nt = w.shape[0] // x.shape[1]
    length = v.shape[0]
    rows = WIDTH // ny
    depth = w.shape[0] // (nz * ny)
    lanes = 2 * WIDTH
    dma = pltpu.SemaphoreType.DMA

    def scan_buffers():
        return [
            pltpu.VMEM((ny, rows, lanes), BF16),
            pltpu.VMEM((ny, rows, lanes), BF16),
            pltpu.VMEM((2, rows, WIDTH), BF16),
            pltpu.VMEM((nz, rows, WIDTH), BF16),
            pltpu.VMEM((ny, rows, lanes), BF16),
            pltpu.VMEM((WIDTH, lanes), BF16),
        ]

    results = (
        ((length, WIDTH), BF16),
        ((length, WIDTH), F32),
        ((length, WIDTH), F32),
        ((length, WIDTH), BF16),
        ((depth, WIDTH), F32),
    )
    near, far = 2 * NEAR, nz - 2 * NEAR - 1
    vmem = pl.BlockSpec(memory_space=pltpu.VMEM)
    anywhere = pl.BlockSpec(memory_space=pl.ANY)
    held = pl.pallas_call(
        functools.partial(kernel, nz, ny, nt),
        out_shape=tuple(pltpu.VMEM(shape, dtype) for shape, dtype in results),
        in_specs=[anywhere] * 9,
        out_specs=[vmem] * 5,
        scratch_shapes=[
            pltpu.VMEM(w.shape, BF16),
            pltpu.VMEM(v.shape, BF16),
            pltpu.VMEM(gf.shape, BF16),
            pltpu.VMEM(gb.shape, BF16),
            pltpu.VMEM(slack.shape, F32),
            pltpu.VMEM((2, 1, length), F32),
            pltpu.VMEM((1, WIDTH), F32),
            pltpu.VMEM(cot.shape, BF16),
            dma((9,)),
            pltpu.VMEM((nt, length, x.shape[1]), BF16),
            pltpu.VMEM((w.shape[0], length), BF16),
            pltpu.VMEM((ny, 1, lanes), F32),
            pltpu.VMEM((nz, 1, lanes), F32),
        ]
        + scan_buffers()
        + scan_buffers()
        + [
            pltpu.VMEM((far + 1, ny, depth, WIDTH), BF16),
            pltpu.VMEM((ny, far + 1, depth, WIDTH), BF16),
            pltpu.VMEM((far + 1, depth, WIDTH), BF16),
            pltpu.VMEM((far, depth, WIDTH), BF16),
            pltpu.VMEM((near, ny, depth, WIDTH), BF16),
            pltpu.VMEM((near, ny, depth, WIDTH), BF16),
            pltpu.VMEM((ny, depth, WIDTH), BF16),
            pltpu.VMEM((ny, depth, WIDTH), BF16),
            dma((nt,)), dma((nt,)), dma((ny,)), dma((ny,)), dma((nz,)), dma((nz,)),
        ]
        + [dma((n,)) for n in (ny, ny, nz, nz, ny, ny)] * 2
        + [dma(n) for n in ((3, ny), (3, ny), (near,), (near,), (ny,), (ny,), (far,), (far,))],
        compiler_params=pltpu.CompilerParams(collective_id=0, has_side_effects=True),
    )(x, w, v, gf, gb, slack, extra.transpose(0, 2, 1), scale.reshape(1, WIDTH), cot)
    return pl.pallas_call(
        store,
        out_shape=tuple(jax.ShapeDtypeStruct(shape, dtype) for shape, dtype in results),
        in_specs=[vmem] * 5,
        out_specs=[anywhere] * 5,
        scratch_shapes=[dma((5,))],
    )(*(in_vmem(a) for a in held))


def solution(mesh):
    torus = Mesh(mesh.devices.reshape(NZ, NY, mesh.shape["tp"]), ("sp_0", "sp_1", "tp"))
    sp = ("sp_0", "sp_1")
    return jax.shard_map(
        functools.partial(on_device, NZ, NY),
        mesh=torus,
        in_specs=(
            P(sp, "tp"),
            P(None, "tp"),
            P(sp, "tp"),
            P(sp, "tp"),
            P(sp, "tp"),
            P(None, "tp"),
            P(None, sp, "tp"),
            P("tp"),
            P(sp, "tp"),
        ),
        out_specs=(P(sp, "tp"),) * 5,
        check_vma=False,
    )
```

```python
import functools

import jax
import jax.numpy as jnp
from jax import lax
from jax.experimental import pallas as pl
from jax.experimental.pallas import tpu as pltpu
from jax.sharding import Mesh
from jax.sharding import PartitionSpec as P

WIDTH = 128
HALF = 128
NZ, NY = 12, 8
NEAR = 3
GROUPS = (2, 1)
EARLY = 1
EPS = 1e-6
MESH_ID = pl.DeviceIdType.MESH
F32, BF16 = jnp.float32, jnp.bfloat16

NN = (((1,), (0,)), ((), ()))
NT = (((1,), (1,)), ((), ()))
TN = (((0,), (0,)), ((), ()))


def dot(a, b, dims):
    a, b = (p if isinstance(p, tuple) else (p,) for p in (a, b))
    total = lax.dot_general(a[0], b[0], dims, preferred_element_type=F32)
    for tail in a[1:]:
        total += lax.dot_general(tail, b[0], dims, preferred_element_type=F32)
    for tail in b[1:]:
        total += lax.dot_general(a[0], tail, dims, preferred_element_type=F32)
    return total


def pair_of(x):
    head = x.astype(BF16)
    return head, (x - head.astype(F32)).astype(BF16)


def cut(pair, *at):
    return tuple(part[at] for part in pair)


def pieces(x, count):
    parts = []
    for _ in range(count):
        part = x.astype(BF16)
        parts.append(part)
        x = x - part.astype(F32)
    return parts


def summed(triangle, x, count):
    return sum(dot(triangle, part, NN) for part in pieces(x, count))


def both(x):
    return jnp.concatenate([x, x], axis=1)


def swapped(x):
    return jnp.concatenate([x[:, WIDTH:], x[:, :WIDTH]], axis=1)


def remote(src, dst, send, recv, peer):
    return pltpu.make_async_remote_copy(
        src_ref=src, dst_ref=dst, send_sem=send, recv_sem=recv, device_id=peer, device_id_type=MESH_ID
    )


EXCHANGES = ("dy", "a1", "dz", "b1", "c1", "a2", "b2", "c2", "g0", "g1", "g2", "b3", "a4", "b4", "xo", "xf")


def kernel(
    nz, ny, nt,
    x_hbm, w_hbm, v_hbm, gf_hbm, gb_hbm, slack_hbm, extra_hbm, scale_hbm, cot_hbm,
    dq_ref, dgf_ref, dgb_ref, dv_ref, dw_ref,
    w_ref, v_ref, gf_ref, gb_ref, slack_ref, extra_ref, scale_ref, cot_ref, load_sem,
    xall, xturn, dec_y, dec_z,
    out1, in1, mid1, got1, back1, state1,
    out2, in2, mid2, got2, back2, state2,
    wa, wa_in, wa_mid, wa_got, wb, wb_in, wb_mid, wb_got,
    send_sem, recv_sem,
):
    z, y, t = lax.axis_index("sp_0"), lax.axis_index("sp_1"), lax.axis_index("tp")
    rows = WIDTH // ny
    length = v_ref.shape[0]
    width_in = xall.shape[2]

    def far_first(n):
        return sorted(range(1, n), key=lambda o: -min(o, n - o))

    def at_y(o):
        return lax.rem(y + o, ny)

    def at_z(o):
        return lax.rem(z + o, nz)

    partner = t + 1 - 2 * lax.rem(t, 2)
    steps = far_first(nt // 2)
    chips = [lax.rem(t + 2 * o, nt) for o in steps]

    barrier = pltpu.get_barrier_semaphore()
    count = 0
    for o in range(1, nz):
        pl.semaphore_signal(barrier, inc=1, device_id={"sp_0": at_z(o)}, device_id_type=MESH_ID)
        count += 1
    for o in range(1, ny):
        pl.semaphore_signal(barrier, inc=1, device_id={"sp_1": at_y(o)}, device_id_type=MESH_ID)
        count += 1
    for k in [partner] + chips:
        pl.semaphore_signal(barrier, inc=1, device_id={"tp": k}, device_id_type=MESH_ID)
        count += 1

    loads = []
    for i, (src, dst) in enumerate(
        (
            (gf_hbm, gf_ref),
            (gb_hbm, gb_ref),
            (slack_hbm, slack_ref),
            (extra_hbm, extra_ref),
            (v_hbm, v_ref),
            (x_hbm, xall.at[t]),
            (w_hbm, w_ref),
            (cot_hbm, cot_ref),
            (scale_hbm, scale_ref),
        )
    ):
        load = pltpu.make_async_copy(src, dst, load_sem.at[i])
        load.start()
        loads.append(load)

    def send(name, src, dst, peer, chip=None):
        n = EXCHANGES.index(name)
        m = n if chip is None else len(EXCHANGES) + chip
        remote(src, dst, send_sem.at[n], recv_sem.at[m], peer).start()

    def arrived(name, whole, peer, chip=None):
        n = EXCHANGES.index(name)
        m = n if chip is None else len(EXCHANGES) + chip
        remote(whole, whole, send_sem.at[n], recv_sem.at[m], peer).wait_recv()

    def gone(name, whole, peer):
        n = EXCHANGES.index(name)
        remote(whole, whole, send_sem.at[n], recv_sem.at[n], peer).wait_send()

    next_y, next_z = {"sp_1": at_y(1)}, {"sp_0": at_z(1)}
    others_y, others_z = pl.ds(0, ny - 1), pl.ds(0, nz - 1)

    for load in loads[:4]:
        load.wait()
    pre = jnp.concatenate([gf_ref[...], gb_ref[...]], axis=1).astype(F32)
    slack = jnp.concatenate([slack_ref[0:1, :], slack_ref[1:2, :]], axis=1)
    gate = jax.nn.sigmoid(-pre)
    key = slack * gate
    forget = jnp.log1p(-key)
    row_id = lax.broadcasted_iota(jnp.int32, (length, length), 0)
    col_id = lax.broadcasted_iota(jnp.int32, (length, length), 1)
    lower = row_id >= col_id
    upper = row_id <= col_id
    lower_ones = jnp.where(lower, 1.0, 0.0).astype(BF16)
    upper_ones = jnp.where(upper, 1.0, 0.0).astype(BF16)
    spikes_f = jnp.sum(jnp.where(lower, extra_ref[0], 0.0), axis=1, keepdims=True)
    spikes_b = jnp.sum(jnp.where(upper, extra_ref[1], 0.0), axis=1, keepdims=True)
    run = jnp.concatenate(
        [
            summed(lower_ones, forget[:, :WIDTH], 3) + spikes_f,
            summed(upper_ones, forget[:, WIDTH:], 3) + spikes_b,
        ],
        axis=1,
    )
    closing = jnp.concatenate([run[length - 1 :, :WIDTH], run[0:1, WIDTH:]], axis=1)
    to_end = jnp.exp(closing - run)
    key_end = (key * to_end).astype(BF16)
    loads[4].wait()
    v = v_ref[...]
    local = dot(v, key_end, TN)
    out1[...] = local.astype(BF16).reshape(ny, rows, 2 * WIDTH)
    dec_y[pl.ds(y, 1)] = closing[None]
    in1[pl.ds(y, 1)] = out1[pl.ds(y, 1)]

    pl.semaphore_wait(barrier, count)

    def first_phase(name, out, into):
        for o in far_first(ny):
            k = at_y(o)
            send(name, out.at[k], into.at[y], {"sp_1": k})

    def line_fold(into, decays):
        up, down = [None] * ny, [None] * ny
        total = jnp.zeros((rows, WIDTH), F32)
        for k in range(ny):
            up[k] = total
            total = jnp.exp(decays[k][:, :WIDTH]) * total + into[k, :, :WIDTH].astype(F32)
        total_up = total
        total = jnp.zeros((rows, WIDTH), F32)
        for k in reversed(range(ny)):
            down[k] = total
            total = jnp.exp(decays[k][:, WIDTH:]) * total + into[k, :, WIDTH:].astype(F32)
        return up, down, total_up, total

    def second_phase(name, mid, got, totals):
        mid[0] = totals[0].astype(BF16)
        mid[1] = totals[1].astype(BF16)
        got[pl.ds(z, 1)] = jnp.zeros((1, rows, WIDTH), BF16)
        for o in far_first(nz):
            k = at_z(o)
            side = jnp.where(k > z, 0, 1)
            send(name, mid.at[side], got.at[z], {"sp_0": k})

    def line_entry(got, decays):
        above = jnp.zeros((rows, WIDTH), F32)
        for k in range(nz):
            new = jnp.exp(decays[k][:, :WIDTH]) * above + got[k].astype(F32)
            above = jnp.where(k < z, new, above)
        below = jnp.zeros((rows, WIDTH), F32)
        for k in reversed(range(nz)):
            new = jnp.exp(decays[k][:, WIDTH:]) * below + got[k].astype(F32)
            below = jnp.where(k > z, new, below)
        return above, below

    def third_phase(name, back, state, entry, prefixes, decays):
        above, below = entry
        up, down = prefixes
        past = jnp.zeros((1, WIDTH), F32)
        first = []
        for k in range(ny):
            first.append(jnp.exp(past) * above + up[k])
            past = past + decays[k][:, :WIDTH]
        past = jnp.zeros((1, WIDTH), F32)
        second = [None] * ny
        for k in reversed(range(ny)):
            second[k] = jnp.exp(past) * below + down[k]
            past = past + decays[k][:, WIDTH:]
        for k in range(ny):
            back[k] = jnp.concatenate([first[k], second[k]], axis=1).astype(BF16)
        here = pl.ds(pl.multiple_of(y * rows, rows), rows)
        for o in far_first(ny):
            k = at_y(o)
            send(name, back.at[k], state.at[here, :], {"sp_1": k})
        state[here, :] = back[pl.ds(y, 1)].reshape(rows, 2 * WIDTH)

    for o in far_first(ny):
        send("dy", dec_y.at[y], dec_y.at[y], {"sp_1": at_y(o)})
    first_phase("a1", out1, in1)
    loads[5].wait()
    for i, k in enumerate(chips):
        send("xo", xall.at[t], xall.at[t], {"tp": k}, i)
    send("xo", xall.at[t], xall.at[t], {"tp": partner}, len(chips))

    first_half = lax.broadcasted_iota(jnp.int32, (length, 2 * WIDTH), 0) < HALF
    centre = [run[HALF // 2 - 1 : HALF // 2], run[HALF + HALF // 2 - 1 : HALF + HALF // 2]]
    middle = jnp.where(first_half, centre[0], centre[1])
    grow = jnp.exp(run - middle)
    shrink = jnp.exp(middle - run)
    from_start = jnp.exp(run)
    keys = pair_of(key * shrink)
    step_f = jnp.exp(centre[1][:, :WIDTH] - centre[0][:, :WIDTH])
    step_b = jnp.exp(centre[0][:, WIDTH:] - centre[1][:, WIDTH:])

    arrived("dy", dec_y.at[others_y], next_y)
    decays1 = [dec_y[k] for k in range(ny)]
    line_total = sum(decays1[1:], decays1[0])
    dec_z[pl.ds(z, 1)] = line_total[None]
    for o in far_first(nz):
        send("dz", dec_z.at[z], dec_z.at[z], {"sp_0": at_z(o)})
    arrived("a1", in1.at[others_y], next_y)
    up, down, total_up, total_down = line_fold(in1, decays1)
    second_phase("b1", mid1, got1, (total_up, total_down))

    arrived("dz", dec_z.at[others_z], next_z)
    arrived("b1", got1.at[others_z], next_z)
    lines1 = [dec_z[k] for k in range(nz)]
    entry = line_entry(got1, lines1)
    third_phase("c1", back1, state1, entry, (up, down), decays1)

    for o, k in zip(steps, chips):
        arrived("xo", xall.at[k], {"tp": k}, steps.index(nt // 2 - o))
        send("xf", xall.at[k], xall.at[k], {"tp": partner})
    arrived("xo", xall.at[partner], {"tp": partner}, len(chips))
    if chips:
        arrived("xf", xall.at[pl.ds(0, len(chips))], {"tp": partner})
    for load in loads[6:]:
        load.wait()
    raw = jnp.zeros((length, WIDTH), F32)
    for k in range(nt):
        raw += dot(xall[k], w_ref[pl.ds(k * width_in, width_in), :], NN)
    raw = raw.astype(BF16).astype(F32)
    sig = jax.nn.sigmoid(raw)
    root = WIDTH**-0.5
    query = both(raw * sig * root)
    queries = query * grow
    query_in = pair_of(query * from_start)

    lo, hi = slice(0, HALF), slice(HALF, 2 * HALF)
    fw, bw = slice(0, WIDTH), slice(WIDTH, 2 * WIDTH)
    far_f = pair_of(queries[hi, fw] * step_f)
    far_b = pair_of(queries[lo, bw] * step_b)
    queries = pair_of(queries)
    low = lower[lo, lo]
    upp = upper[lo, lo]

    def near(a):
        return jnp.where(low, dot(cut(queries, a, fw), cut(keys, a, fw), NT), 0.0) + jnp.where(
            upp, dot(cut(queries, a, bw), cut(keys, a, bw), NT), 0.0
        )

    scores = jnp.concatenate(
        [
            jnp.concatenate([near(lo), dot(far_b, cut(keys, hi, bw), NT)], axis=1),
            jnp.concatenate([dot(far_f, cut(keys, lo, fw), NT), near(hi)], axis=1),
        ],
        axis=0,
    )
    scores = pair_of(scores)
    inside = dot(scores, v, NN)
    for k in range(nt):
        xturn[pl.ds(k * width_in, width_in), :] = xall[k].T

    arrived("c1", state1.at[pl.ds(0, WIDTH - rows), :], next_y)
    state = state1[...]
    mixed = inside + dot(query_in, state, NT)
    inv = lax.rsqrt(jnp.mean(mixed * mixed, axis=1, keepdims=True) + EPS)
    weighted = cot_ref[...].astype(F32) * scale_ref[...]
    along = jnp.mean(weighted * mixed, axis=1, keepdims=True)
    grad_out = pair_of(inv * (weighted - mixed * (inv * inv * along)))

    sense = dot(grad_out, query_in, TN)
    out2[...] = swapped(sense).astype(BF16).reshape(ny, rows, 2 * WIDTH)
    in2[pl.ds(y, 1)] = out2[pl.ds(y, 1)]
    first_phase("a2", out2, in2)

    cross = dot(grad_out, v, NT)
    cross_low = [pair_of(jnp.where(low, cross[a, a], 0.0)) for a in (lo, hi)]
    cross_upp = [pair_of(jnp.where(upp, cross[a, a], 0.0)) for a in (lo, hi)]
    cross_f, cross_b = pair_of(cross[hi, lo]), pair_of(cross[lo, hi])
    dq_f = jnp.concatenate(
        [
            dot(cross_low[0], cut(keys, lo, fw), NN),
            dot(cross_low[1], cut(keys, hi, fw), NN) + step_f * dot(cross_f, cut(keys, lo, fw), NN),
        ],
        axis=0,
    )
    dq_b = jnp.concatenate(
        [
            dot(cross_upp[0], cut(keys, lo, bw), NN) + step_b * dot(cross_b, cut(keys, hi, bw), NN),
            dot(cross_upp[1], cut(keys, hi, bw), NN),
        ],
        axis=0,
    )
    dq = grow * jnp.concatenate([dq_f, dq_b], axis=1) + from_start * dot(grad_out, state, NN)
    draw = (dq[:, fw] + dq[:, bw]) * (root * sig * (1.0 + raw * (1.0 - sig)))
    draw = draw.astype(BF16)
    dq_ref[...] = draw

    part = ny * wa.shape[2]
    far, near = nz - 2 * NEAR - 1, 2 * NEAR
    far_turn = sum(jnp.where(z + NEAR + 1 + i < nz, 1, 0) for i in range(far))
    near_at = [i + 1 + (nz - 1 - 2 * NEAR) * (i // NEAR) for i in range(near)]
    near_turn = sum(jnp.where(z + o < nz, 1, 0) for o in near_at)
    first, second = GROUPS
    slots = [*range(first + second), None, *range(first + second, far)]
    groups = [slice(0, first), slice(first, first + second + 1), slice(first + second + 1, far + 1)]

    def far_index(rank):
        return lax.rem(far_turn + rank, far)

    def far_owner(index):
        return lax.rem(z + NEAR + 1 + index, nz)

    def terms(owner):
        start = pl.multiple_of(owner * part, part)
        return dot(xturn[pl.ds(start, part), :], draw, NN).astype(BF16).reshape(wa.shape[1:])

    def far_send(g):
        for o in far_first(ny):
            k = at_y(o)
            send(f"g{g}", wa.at[groups[g], k], wa_in.at[y, groups[g]], {"sp_1": k})

    def far_pass(g):
        arrived(f"g{g}", wa_in.at[others_y, groups[g]], next_y)
        count = groups[g].stop - groups[g].start
        acc = wa[groups[g], pl.ds(y, 1)].astype(F32).reshape(count, *wa_mid.shape[1:])
        for o in range(1, ny):
            acc += wa_in[pl.ds(at_y(o), 1), groups[g]].astype(F32).reshape(acc.shape)
        wa_mid[groups[g]] = acc.astype(BF16)
        kept = None
        for n, rank in enumerate(slots[groups[g]]):
            slot = groups[g].start + n
            if rank is None:
                kept = acc[n]
            else:
                i = far_index(rank)
                send("b4", wa_mid.at[slot], wa_got.at[i], {"sp_0": far_owner(i)})
        return kept

    def fill(g):
        for slot in range(groups[g].start, groups[g].stop):
            wa[slot] = terms(z if slots[slot] is None else far_owner(far_index(slots[slot])))

    def near_send(ranks):
        for rank in ranks:
            i = lax.rem(near_turn + rank, near)
            o = i + 1 + (nz - 1 - 2 * NEAR) * (i // NEAR)
            send("b3", wb.at[i], wb_in.at[i], {"sp_0": lax.rem(z + o, nz)})

    def near_fill(ranks):
        for rank in ranks:
            i = lax.rem(near_turn + rank, near)
            o = i + 1 + (nz - 1 - 2 * NEAR) * (i // NEAR)
            wb[pl.ds(i, 1)] = terms(lax.rem(z + o, nz))[None]

    fill(0)
    far_send(0)
    near_fill(range(EARLY))
    near_send(range(EARLY))
    fill(1)
    far_send(1)
    fill(2)
    far_send(2)
    near_fill(range(EARLY, near))

    decays2 = [swapped(d) for d in decays1]
    lines2 = [swapped(d) for d in lines1]
    arrived("a2", in2.at[others_y], next_y)
    up, down, total_up, total_down = line_fold(in2, decays2)
    second_phase("b2", mid2, got2, (total_up, total_down))
    near_send(range(EARLY, near))

    dv = dot(scores, grad_out, TN)
    dk_f = jnp.concatenate(
        [
            dot(cross_low[0], cut(queries, lo, fw), TN) + dot(cross_f, far_f, TN),
            dot(cross_low[1], cut(queries, hi, fw), TN),
        ],
        axis=0,
    )
    dk_b = jnp.concatenate(
        [
            dot(cross_upp[0], cut(queries, lo, bw), TN),
            dot(cross_upp[1], cut(queries, hi, bw), TN) + dot(cross_b, far_b, TN),
        ],
        axis=0,
    )
    dk = shrink * jnp.concatenate([dk_f, dk_b], axis=1)
    drift = query * dq - key * dk
    left = jnp.exp(closing) * state.astype(F32) + local

    far_pass(0)
    arrived("b2", got2.at[others_z], next_z)
    entry = line_entry(got2, lines2)
    third_phase("c2", back2, state2, entry, (up, down), decays2)

    own = far_pass(1)
    far_pass(2)
    arrived("b3", wb_in, next_z)
    acc = wb_in[0].astype(F32)
    for i in range(1, near):
        acc += wb_in[i].astype(F32)
    wb_mid[...] = acc.astype(BF16)
    for o in far_first(ny):
        k = at_y(o)
        send("a4", wb_mid.at[k], wb_got.at[y], {"sp_1": k})
    own += wb_mid[pl.ds(y, 1)].astype(F32).reshape(dw_ref.shape)

    arrived("c2", state2.at[pl.ds(0, WIDTH - rows), :], next_y)
    after = swapped(state2[...])
    dv_ref[...] = (dv + dot(key_end, after, NT)).astype(BF16)
    dk_end = to_end * dot(v, after, NN)
    ends = jnp.sum(after.astype(F32) * left, axis=0, keepdims=True)
    drift = drift - key * dk_end
    drift = jnp.concatenate(
        [summed(upper_ones, drift[:, fw], 2), summed(lower_ones, drift[:, bw], 2)], axis=1
    )
    dkey = dk + dk_end - (drift + ends) / (1.0 - key)
    dgate = -key * (1.0 - gate) * dkey
    dgf_ref[...] = dgate[:, fw]
    dgb_ref[...] = dgate[:, bw]

    arrived("a4", wb_got.at[others_y], next_y)
    for o in range(1, ny):
        own += wb_got[pl.ds(at_y(o), 1)].astype(F32).reshape(own.shape)
    arrived("b4", wa_got, next_z)
    for i in range(far):
        own += wa_got[i].astype(F32)
    dw_ref[...] = own

    for name, whole in (
        ("dy", dec_y.at[others_y]),
        ("a1", out1.at[others_y]),
        ("c1", back1.at[others_y]),
        ("a2", out2.at[others_y]),
        ("c2", back2.at[others_y]),
        ("g0", wa_in.at[others_y, groups[0]]),
        ("g1", wa_in.at[others_y, groups[1]]),
        ("g2", wa_in.at[others_y, groups[2]]),
        ("a4", wb_got.at[others_y]),
    ):
        gone(name, whole, next_y)
    for name, whole in (
        ("dz", dec_z.at[others_z]),
        ("b1", got1.at[others_z]),
        ("b2", got2.at[others_z]),
        ("b3", wb_in),
        ("b4", wa_got),
    ):
        gone(name, whole, next_z)
    gone("xo", xall.at[pl.ds(0, len(chips) + 1)], {"tp": partner})
    if chips:
        gone("xf", xall.at[pl.ds(0, len(chips))], {"tp": partner})


def store(*refs):
    sources, targets, sems = refs[:5], refs[5:10], refs[10]
    copies = [
        pltpu.make_async_copy(src, dst, sems.at[i])
        for i, (src, dst) in enumerate(zip(sources, targets))
    ]
    for copy in copies:
        copy.start()
    for copy in copies:
        copy.wait()


def in_vmem(a):
    return pltpu.with_memory_space_constraint(a, pltpu.VMEM)


def on_device(nz, ny, x, w, v, gf, gb, slack, extra, scale, cot):
    nt = w.shape[0] // x.shape[1]
    length = v.shape[0]
    rows = WIDTH // ny
    depth = w.shape[0] // (nz * ny)
    lanes = 2 * WIDTH
    dma = pltpu.SemaphoreType.DMA

    def scan_buffers():
        return [
            pltpu.VMEM((ny, rows, lanes), BF16),
            pltpu.VMEM((ny, rows, lanes), BF16),
            pltpu.VMEM((2, rows, WIDTH), BF16),
            pltpu.VMEM((nz, rows, WIDTH), BF16),
            pltpu.VMEM((ny, rows, lanes), BF16),
            pltpu.VMEM((WIDTH, lanes), BF16),
        ]

    results = (
        ((length, WIDTH), BF16),
        ((length, WIDTH), F32),
        ((length, WIDTH), F32),
        ((length, WIDTH), BF16),
        ((depth, WIDTH), F32),
    )
    near, far = 2 * NEAR, nz - 2 * NEAR - 1
    vmem = pl.BlockSpec(memory_space=pltpu.VMEM)
    anywhere = pl.BlockSpec(memory_space=pl.ANY)
    held = pl.pallas_call(
        functools.partial(kernel, nz, ny, nt),
        out_shape=tuple(pltpu.VMEM(shape, dtype) for shape, dtype in results),
        in_specs=[anywhere] * 9,
        out_specs=[vmem] * 5,
        scratch_shapes=[
            pltpu.VMEM(w.shape, BF16),
            pltpu.VMEM(v.shape, BF16),
            pltpu.VMEM(gf.shape, BF16),
            pltpu.VMEM(gb.shape, BF16),
            pltpu.VMEM(slack.shape, F32),
            pltpu.VMEM((2, 1, length), F32),
            pltpu.VMEM((1, WIDTH), F32),
            pltpu.VMEM(cot.shape, BF16),
            dma((9,)),
            pltpu.VMEM((nt, length, x.shape[1]), BF16),
            pltpu.VMEM((w.shape[0], length), BF16),
            pltpu.VMEM((ny, 1, lanes), F32),
            pltpu.VMEM((nz, 1, lanes), F32),
        ]
        + scan_buffers()
        + scan_buffers()
        + [
            pltpu.VMEM((far + 1, ny, depth, WIDTH), BF16),
            pltpu.VMEM((ny, far + 1, depth, WIDTH), BF16),
            pltpu.VMEM((far + 1, depth, WIDTH), BF16),
            pltpu.VMEM((far, depth, WIDTH), BF16),
            pltpu.VMEM((near, ny, depth, WIDTH), BF16),
            pltpu.VMEM((near, ny, depth, WIDTH), BF16),
            pltpu.VMEM((ny, depth, WIDTH), BF16),
            pltpu.VMEM((ny, depth, WIDTH), BF16),
            dma((len(EXCHANGES),)),
            dma((len(EXCHANGES) + nt // 2,)),
        ],
        compiler_params=pltpu.CompilerParams(collective_id=0, has_side_effects=True),
    )(x, w, v, gf, gb, slack, extra.transpose(0, 2, 1), scale.reshape(1, WIDTH), cot)
    return pl.pallas_call(
        store,
        out_shape=tuple(jax.ShapeDtypeStruct(shape, dtype) for shape, dtype in results),
        in_specs=[vmem] * 5,
        out_specs=[anywhere] * 5,
        scratch_shapes=[dma((5,))],
    )(*(in_vmem(a) for a in held))


def solution(mesh):
    torus = Mesh(mesh.devices.reshape(NZ, NY, mesh.shape["tp"]), ("sp_0", "sp_1", "tp"))
    sp = ("sp_0", "sp_1")
    return jax.shard_map(
        functools.partial(on_device, NZ, NY),
        mesh=torus,
        in_specs=(
            P(sp, "tp"),
            P(None, "tp"),
            P(sp, "tp"),
            P(sp, "tp"),
            P(sp, "tp"),
            P(None, "tp"),
            P(None, sp, "tp"),
            P("tp"),
            P(sp, "tp"),
        ),
        out_specs=(P(sp, "tp"),) * 5,
        check_vma=False,
    )
```

```python
import functools

import jax
import jax.numpy as jnp
from jax import lax
from jax.experimental import pallas as pl
from jax.experimental.pallas import tpu as pltpu
from jax.sharding import Mesh
from jax.sharding import PartitionSpec as P

WIDTH = 128
HALF = 128
NZ, NY = 12, 8
NEAR = 3
GROUPS = (2, 1)
EARLY, MIDDLE = 1, 3
EPS = 1e-6
MESH_ID = pl.DeviceIdType.MESH
F32, BF16 = jnp.float32, jnp.bfloat16

NN = (((1,), (0,)), ((), ()))
NT = (((1,), (1,)), ((), ()))
TN = (((0,), (0,)), ((), ()))


def dot(a, b, dims):
    a, b = (p if isinstance(p, tuple) else (p,) for p in (a, b))
    total = lax.dot_general(a[0], b[0], dims, preferred_element_type=F32)
    for tail in a[1:]:
        total += lax.dot_general(tail, b[0], dims, preferred_element_type=F32)
    for tail in b[1:]:
        total += lax.dot_general(a[0], tail, dims, preferred_element_type=F32)
    return total


def pair_of(x):
    head = x.astype(BF16)
    return head, (x - head.astype(F32)).astype(BF16)


def cut(pair, *at):
    return tuple(part[at] for part in pair)


def pieces(x, count):
    parts = []
    for _ in range(count):
        part = x.astype(BF16)
        parts.append(part)
        x = x - part.astype(F32)
    return parts


def summed(triangle, x, count):
    return sum(dot(triangle, part, NN) for part in pieces(x, count))


def both(x):
    return jnp.concatenate([x, x], axis=1)


def swapped(x):
    return jnp.concatenate([x[:, WIDTH:], x[:, :WIDTH]], axis=1)


def remote(src, dst, send, recv, peer):
    return pltpu.make_async_remote_copy(
        src_ref=src, dst_ref=dst, send_sem=send, recv_sem=recv, device_id=peer, device_id_type=MESH_ID
    )


EXCHANGES = ("dy", "a1", "dz", "b1", "c1", "a2", "b2", "c2", "g0", "g1", "g2", "b3", "a4", "b4", "xo", "xf")


def kernel(
    nz, ny, nt,
    x_hbm, w_hbm, v_hbm, gf_hbm, gb_hbm, slack_hbm, extra_hbm, scale_hbm, cot_hbm,
    dq_ref, dgf_ref, dgb_ref, dv_ref, dw_ref,
    w_ref, v_ref, gf_ref, gb_ref, slack_ref, extra_ref, scale_ref, cot_ref, load_sem,
    xall, xturn, dec_y, dec_z,
    out1, in1, mid1, got1, back1, state1,
    out2, in2, mid2, got2, back2, state2,
    wa, wa_in, wa_mid, wa_got, wb, wb_in, wb_mid, wb_got,
    send_sem, recv_sem,
):
    z, y, t = lax.axis_index("sp_0"), lax.axis_index("sp_1"), lax.axis_index("tp")
    rows = WIDTH // ny
    length = v_ref.shape[0]
    width_in = xall.shape[2]

    def far_first(n):
        return sorted(range(1, n), key=lambda o: -min(o, n - o))

    def at_y(o):
        return lax.rem(y + o, ny)

    def at_z(o):
        return lax.rem(z + o, nz)

    partner = t + 1 - 2 * lax.rem(t, 2)
    steps = far_first(nt // 2)
    chips = [lax.rem(t + 2 * o, nt) for o in steps]

    loads = []
    for i, (src, dst) in enumerate(
        (
            (gf_hbm, gf_ref),
            (gb_hbm, gb_ref),
            (slack_hbm, slack_ref),
            (extra_hbm, extra_ref),
            (v_hbm, v_ref),
            (x_hbm, xall.at[t]),
            (w_hbm, w_ref),
            (cot_hbm, cot_ref),
            (scale_hbm, scale_ref),
        )
    ):
        load = pltpu.make_async_copy(src, dst, load_sem.at[i])
        load.start()
        loads.append(load)

    barrier = pltpu.get_barrier_semaphore()
    count = 0
    for o in far_first(nz):
        pl.semaphore_signal(barrier, inc=1, device_id={"sp_0": at_z(o)}, device_id_type=MESH_ID)
        count += 1
    for o in range(1, ny):
        pl.semaphore_signal(barrier, inc=1, device_id={"sp_1": at_y(o)}, device_id_type=MESH_ID)
        count += 1
    for k in [partner] + chips:
        pl.semaphore_signal(barrier, inc=1, device_id={"tp": k}, device_id_type=MESH_ID)
        count += 1

    def send(name, src, dst, peer, chip=None):
        n = EXCHANGES.index(name)
        m = n if chip is None else len(EXCHANGES) + chip
        remote(src, dst, send_sem.at[n], recv_sem.at[m], peer).start()

    def arrived(name, whole, peer, chip=None):
        n = EXCHANGES.index(name)
        m = n if chip is None else len(EXCHANGES) + chip
        remote(whole, whole, send_sem.at[n], recv_sem.at[m], peer).wait_recv()

    def gone(name, whole, peer):
        n = EXCHANGES.index(name)
        remote(whole, whole, send_sem.at[n], recv_sem.at[n], peer).wait_send()

    next_y, next_z = {"sp_1": at_y(1)}, {"sp_0": at_z(1)}
    others_y, others_z = pl.ds(0, ny - 1), pl.ds(0, nz - 1)

    for load in loads[:4]:
        load.wait()
    pre = jnp.concatenate([gf_ref[...], gb_ref[...]], axis=1).astype(F32)
    slack = jnp.concatenate([slack_ref[0:1, :], slack_ref[1:2, :]], axis=1)
    gate = jax.nn.sigmoid(-pre)
    key = slack * gate
    forget = jnp.log1p(-key)
    row_id = lax.broadcasted_iota(jnp.int32, (length, length), 0)
    col_id = lax.broadcasted_iota(jnp.int32, (length, length), 1)
    lower = row_id >= col_id
    upper = row_id <= col_id
    lower_ones = jnp.where(lower, 1.0, 0.0).astype(BF16)
    upper_ones = jnp.where(upper, 1.0, 0.0).astype(BF16)
    spikes_f = jnp.sum(jnp.where(lower, extra_ref[0], 0.0), axis=1, keepdims=True)
    spikes_b = jnp.sum(jnp.where(upper, extra_ref[1], 0.0), axis=1, keepdims=True)
    run = jnp.concatenate(
        [
            summed(lower_ones, forget[:, :WIDTH], 3) + spikes_f,
            summed(upper_ones, forget[:, WIDTH:], 3) + spikes_b,
        ],
        axis=1,
    )
    closing = jnp.concatenate([run[length - 1 :, :WIDTH], run[0:1, WIDTH:]], axis=1)
    to_end = jnp.exp(closing - run)
    key_end = (key * to_end).astype(BF16)
    loads[4].wait()
    v = v_ref[...]
    local = dot(v, key_end, TN)
    out1[...] = local.astype(BF16).reshape(ny, rows, 2 * WIDTH)
    dec_y[pl.ds(y, 1)] = closing[None]
    in1[pl.ds(y, 1)] = out1[pl.ds(y, 1)]

    pl.semaphore_wait(barrier, count)

    def first_phase(name, out, into):
        for o in far_first(ny):
            k = at_y(o)
            send(name, out.at[k], into.at[y], {"sp_1": k})

    def line_fold(into, decays):
        up, down = [None] * ny, [None] * ny
        total = jnp.zeros((rows, WIDTH), F32)
        for k in range(ny):
            up[k] = total
            total = jnp.exp(decays[k][:, :WIDTH]) * total + into[k, :, :WIDTH].astype(F32)
        total_up = total
        total = jnp.zeros((rows, WIDTH), F32)
        for k in reversed(range(ny)):
            down[k] = total
            total = jnp.exp(decays[k][:, WIDTH:]) * total + into[k, :, WIDTH:].astype(F32)
        return up, down, total_up, total

    def second_phase(name, mid, got, totals):
        mid[0] = totals[0].astype(BF16)
        mid[1] = totals[1].astype(BF16)
        got[pl.ds(z, 1)] = jnp.zeros((1, rows, WIDTH), BF16)
        for o in far_first(nz):
            k = at_z(o)
            side = jnp.where(k > z, 0, 1)
            send(name, mid.at[side], got.at[z], {"sp_0": k})

    def line_entry(got, decays):
        above = jnp.zeros((rows, WIDTH), F32)
        for k in range(nz):
            new = jnp.exp(decays[k][:, :WIDTH]) * above + got[k].astype(F32)
            above = jnp.where(k < z, new, above)
        below = jnp.zeros((rows, WIDTH), F32)
        for k in reversed(range(nz)):
            new = jnp.exp(decays[k][:, WIDTH:]) * below + got[k].astype(F32)
            below = jnp.where(k > z, new, below)
        return above, below

    def third_phase(name, back, state, entry, prefixes, decays):
        above, below = entry
        up, down = prefixes
        past = jnp.zeros((1, WIDTH), F32)
        first = []
        for k in range(ny):
            first.append(jnp.exp(past) * above + up[k])
            past = past + decays[k][:, :WIDTH]
        past = jnp.zeros((1, WIDTH), F32)
        second = [None] * ny
        for k in reversed(range(ny)):
            second[k] = jnp.exp(past) * below + down[k]
            past = past + decays[k][:, WIDTH:]
        for k in range(ny):
            back[k] = jnp.concatenate([first[k], second[k]], axis=1).astype(BF16)
        here = pl.ds(pl.multiple_of(y * rows, rows), rows)
        for o in far_first(ny):
            k = at_y(o)
            send(name, back.at[k], state.at[here, :], {"sp_1": k})
        state[here, :] = back[pl.ds(y, 1)].reshape(rows, 2 * WIDTH)

    for o in far_first(ny):
        send("dy", dec_y.at[y], dec_y.at[y], {"sp_1": at_y(o)})
    first_phase("a1", out1, in1)
    loads[5].wait()
    for i, k in enumerate(chips):
        send("xo", xall.at[t], xall.at[t], {"tp": k}, i)
    send("xo", xall.at[t], xall.at[t], {"tp": partner}, len(chips))

    first_half = lax.broadcasted_iota(jnp.int32, (length, 2 * WIDTH), 0) < HALF
    centre = [run[HALF // 2 - 1 : HALF // 2], run[HALF + HALF // 2 - 1 : HALF + HALF // 2]]
    middle = jnp.where(first_half, centre[0], centre[1])
    grow = jnp.exp(run - middle)
    shrink = jnp.exp(middle - run)
    from_start = jnp.exp(run)
    keys = pair_of(key * shrink)
    step_f = jnp.exp(centre[1][:, :WIDTH] - centre[0][:, :WIDTH])
    step_b = jnp.exp(centre[0][:, WIDTH:] - centre[1][:, WIDTH:])

    arrived("dy", dec_y.at[others_y], next_y)
    decays1 = [dec_y[k] for k in range(ny)]
    line_total = sum(decays1[1:], decays1[0])
    dec_z[pl.ds(z, 1)] = line_total[None]
    for o in far_first(nz):
        send("dz", dec_z.at[z], dec_z.at[z], {"sp_0": at_z(o)})
    arrived("a1", in1.at[others_y], next_y)
    up, down, total_up, total_down = line_fold(in1, decays1)
    second_phase("b1", mid1, got1, (total_up, total_down))

    arrived("dz", dec_z.at[others_z], next_z)
    arrived("b1", got1.at[others_z], next_z)
    lines1 = [dec_z[k] for k in range(nz)]
    entry = line_entry(got1, lines1)
    third_phase("c1", back1, state1, entry, (up, down), decays1)

    for o, k in zip(steps, chips):
        arrived("xo", xall.at[k], {"tp": k}, steps.index(nt // 2 - o))
        send("xf", xall.at[k], xall.at[k], {"tp": partner})
    arrived("xo", xall.at[partner], {"tp": partner}, len(chips))
    if chips:
        arrived("xf", xall.at[pl.ds(0, len(chips))], {"tp": partner})
    for load in loads[6:]:
        load.wait()
    raw = jnp.zeros((length, WIDTH), F32)
    for k in range(nt):
        raw += dot(xall[k], w_ref[pl.ds(k * width_in, width_in), :], NN)
    raw = raw.astype(BF16).astype(F32)
    sig = jax.nn.sigmoid(raw)
    root = WIDTH**-0.5
    query = both(raw * sig * root)
    queries = query * grow
    query_in = pair_of(query * from_start)

    lo, hi = slice(0, HALF), slice(HALF, 2 * HALF)
    fw, bw = slice(0, WIDTH), slice(WIDTH, 2 * WIDTH)
    far_f = pair_of(queries[hi, fw] * step_f)
    far_b = pair_of(queries[lo, bw] * step_b)
    queries = pair_of(queries)
    low = lower[lo, lo]
    upp = upper[lo, lo]

    def near(a):
        return jnp.where(low, dot(cut(queries, a, fw), cut(keys, a, fw), NT), 0.0) + jnp.where(
            upp, dot(cut(queries, a, bw), cut(keys, a, bw), NT), 0.0
        )

    scores = jnp.concatenate(
        [
            jnp.concatenate([near(lo), dot(far_b, cut(keys, hi, bw), NT)], axis=1),
            jnp.concatenate([dot(far_f, cut(keys, lo, fw), NT), near(hi)], axis=1),
        ],
        axis=0,
    )
    scores = pair_of(scores)
    inside = dot(scores, v, NN)
    for k in range(nt):
        xturn[pl.ds(k * width_in, width_in), :] = xall[k].T

    arrived("c1", state1.at[pl.ds(0, WIDTH - rows), :], next_y)
    state = state1[...]
    mixed = inside + dot(query_in, state, NT)
    inv = lax.rsqrt(jnp.mean(mixed * mixed, axis=1, keepdims=True) + EPS)
    weighted = cot_ref[...].astype(F32) * scale_ref[...]
    along = jnp.mean(weighted * mixed, axis=1, keepdims=True)
    grad_out = pair_of(inv * (weighted - mixed * (inv * inv * along)))

    sense = dot(grad_out, query_in, TN)
    out2[...] = swapped(sense).astype(BF16).reshape(ny, rows, 2 * WIDTH)
    in2[pl.ds(y, 1)] = out2[pl.ds(y, 1)]
    first_phase("a2", out2, in2)

    cross = dot(grad_out, v, NT)
    cross_low = [pair_of(jnp.where(low, cross[a, a], 0.0)) for a in (lo, hi)]
    cross_upp = [pair_of(jnp.where(upp, cross[a, a], 0.0)) for a in (lo, hi)]
    cross_f, cross_b = pair_of(cross[hi, lo]), pair_of(cross[lo, hi])
    dq_f = jnp.concatenate(
        [
            dot(cross_low[0], cut(keys, lo, fw), NN),
            dot(cross_low[1], cut(keys, hi, fw), NN) + step_f * dot(cross_f, cut(keys, lo, fw), NN),
        ],
        axis=0,
    )
    dq_b = jnp.concatenate(
        [
            dot(cross_upp[0], cut(keys, lo, bw), NN) + step_b * dot(cross_b, cut(keys, hi, bw), NN),
            dot(cross_upp[1], cut(keys, hi, bw), NN),
        ],
        axis=0,
    )
    dq = grow * jnp.concatenate([dq_f, dq_b], axis=1) + from_start * dot(grad_out, state, NN)
    draw = (dq[:, fw] + dq[:, bw]) * (root * sig * (1.0 + raw * (1.0 - sig)))
    draw = draw.astype(BF16)
    dq_ref[...] = draw

    part = ny * wa.shape[2]
    far, near = nz - 2 * NEAR - 1, 2 * NEAR
    far_turn = sum(jnp.where(z + NEAR + 1 + i < nz, 1, 0) for i in range(far))
    near_at = [i + 1 + (nz - 1 - 2 * NEAR) * (i // NEAR) for i in range(near)]
    near_turn = sum(jnp.where(z + o < nz, 1, 0) for o in near_at)
    first, second = GROUPS
    slots = [*range(first + second), None, *range(first + second, far)]
    groups = [slice(0, first), slice(first, first + second + 1), slice(first + second + 1, far + 1)]

    def far_index(rank):
        return lax.rem(far_turn + rank, far)

    def far_owner(index):
        return lax.rem(z + NEAR + 1 + index, nz)

    def terms(owner):
        start = pl.multiple_of(owner * part, part)
        return dot(xturn[pl.ds(start, part), :], draw, NN).astype(BF16).reshape(wa.shape[1:])

    def far_send(g):
        for o in far_first(ny):
            k = at_y(o)
            send(f"g{g}", wa.at[groups[g], k], wa_in.at[y, groups[g]], {"sp_1": k})

    def far_pass(g):
        arrived(f"g{g}", wa_in.at[others_y, groups[g]], next_y)
        count = groups[g].stop - groups[g].start
        acc = wa[groups[g], pl.ds(y, 1)].astype(F32).reshape(count, *wa_mid.shape[1:])
        for o in range(1, ny):
            acc += wa_in[pl.ds(at_y(o), 1), groups[g]].astype(F32).reshape(acc.shape)
        wa_mid[groups[g]] = acc.astype(BF16)
        kept = None
        for n, rank in enumerate(slots[groups[g]]):
            slot = groups[g].start + n
            if rank is None:
                kept = acc[n]
            else:
                i = far_index(rank)
                send("b4", wa_mid.at[slot], wa_got.at[i], {"sp_0": far_owner(i)})
        return kept

    def fill(g):
        for slot in range(groups[g].start, groups[g].stop):
            wa[slot] = terms(z if slots[slot] is None else far_owner(far_index(slots[slot])))

    def near_send(ranks):
        for rank in ranks:
            i = lax.rem(near_turn + rank, near)
            o = i + 1 + (nz - 1 - 2 * NEAR) * (i // NEAR)
            send("b3", wb.at[i], wb_in.at[i], {"sp_0": lax.rem(z + o, nz)})

    def near_fill(ranks):
        for rank in ranks:
            i = lax.rem(near_turn + rank, near)
            o = i + 1 + (nz - 1 - 2 * NEAR) * (i // NEAR)
            wb[pl.ds(i, 1)] = terms(lax.rem(z + o, nz))[None]

    fill(0)
    far_send(0)
    near_fill(range(EARLY))
    near_send(range(EARLY))
    fill(1)
    far_send(1)
    fill(2)
    far_send(2)
    near_fill(range(EARLY, near))

    decays2 = [swapped(d) for d in decays1]
    lines2 = [swapped(d) for d in lines1]
    arrived("a2", in2.at[others_y], next_y)
    up, down, total_up, total_down = line_fold(in2, decays2)
    second_phase("b2", mid2, got2, (total_up, total_down))
    near_send(range(EARLY, MIDDLE))

    dv = dot(scores, grad_out, TN)
    dk_f = jnp.concatenate(
        [
            dot(cross_low[0], cut(queries, lo, fw), TN) + dot(cross_f, far_f, TN),
            dot(cross_low[1], cut(queries, hi, fw), TN),
        ],
        axis=0,
    )
    dk_b = jnp.concatenate(
        [
            dot(cross_upp[0], cut(queries, lo, bw), TN),
            dot(cross_upp[1], cut(queries, hi, bw), TN) + dot(cross_b, far_b, TN),
        ],
        axis=0,
    )
    dk = shrink * jnp.concatenate([dk_f, dk_b], axis=1)
    drift = query * dq - key * dk
    left = jnp.exp(closing) * state.astype(F32) + local

    far_pass(0)
    near_send(range(MIDDLE, near))
    arrived("b2", got2.at[others_z], next_z)
    entry = line_entry(got2, lines2)
    third_phase("c2", back2, state2, entry, (up, down), decays2)

    own = far_pass(1)
    far_pass(2)
    arrived("b3", wb_in, next_z)
    acc = wb_in[0].astype(F32)
    for i in range(1, near):
        acc += wb_in[i].astype(F32)
    wb_mid[...] = acc.astype(BF16)
    for o in far_first(ny):
        k = at_y(o)
        send("a4", wb_mid.at[k], wb_got.at[y], {"sp_1": k})
    own += wb_mid[pl.ds(y, 1)].astype(F32).reshape(dw_ref.shape)

    arrived("c2", state2.at[pl.ds(0, WIDTH - rows), :], next_y)
    after = swapped(state2[...])
    dv_ref[...] = (dv + dot(key_end, after, NT)).astype(BF16)
    dk_end = to_end * dot(v, after, NN)
    ends = jnp.sum(after.astype(F32) * left, axis=0, keepdims=True)
    drift = drift - key * dk_end
    drift = jnp.concatenate(
        [summed(upper_ones, drift[:, fw], 2), summed(lower_ones, drift[:, bw], 2)], axis=1
    )
    dkey = dk + dk_end - (drift + ends) / (1.0 - key)
    dgate = -key * (1.0 - gate) * dkey
    dgf_ref[...] = dgate[:, fw]
    dgb_ref[...] = dgate[:, bw]

    arrived("a4", wb_got.at[others_y], next_y)
    for o in range(1, ny):
        own += wb_got[pl.ds(at_y(o), 1)].astype(F32).reshape(own.shape)
    arrived("b4", wa_got, next_z)
    for i in range(far):
        own += wa_got[i].astype(F32)
    dw_ref[...] = own

    for name, whole in (
        ("dy", dec_y.at[others_y]),
        ("a1", out1.at[others_y]),
        ("c1", back1.at[others_y]),
        ("a2", out2.at[others_y]),
        ("c2", back2.at[others_y]),
        ("g0", wa_in.at[others_y, groups[0]]),
        ("g1", wa_in.at[others_y, groups[1]]),
        ("g2", wa_in.at[others_y, groups[2]]),
        ("a4", wb_got.at[others_y]),
    ):
        gone(name, whole, next_y)
    for name, whole in (
        ("dz", dec_z.at[others_z]),
        ("b1", got1.at[others_z]),
        ("b2", got2.at[others_z]),
        ("b3", wb_in),
        ("b4", wa_got),
    ):
        gone(name, whole, next_z)
    gone("xo", xall.at[pl.ds(0, len(chips) + 1)], {"tp": partner})
    if chips:
        gone("xf", xall.at[pl.ds(0, len(chips))], {"tp": partner})


def store(*refs):
    sources, targets, sems = refs[:5], refs[5:10], refs[10]
    copies = [
        pltpu.make_async_copy(src, dst, sems.at[i])
        for i, (src, dst) in enumerate(zip(sources, targets))
    ]
    for copy in copies:
        copy.start()
    for copy in copies:
        copy.wait()


def in_vmem(a):
    return pltpu.with_memory_space_constraint(a, pltpu.VMEM)


def on_device(nz, ny, x, w, v, gf, gb, slack, extra, scale, cot):
    nt = w.shape[0] // x.shape[1]
    length = v.shape[0]
    rows = WIDTH // ny
    depth = w.shape[0] // (nz * ny)
    lanes = 2 * WIDTH
    dma = pltpu.SemaphoreType.DMA

    def scan_buffers():
        return [
            pltpu.VMEM((ny, rows, lanes), BF16),
            pltpu.VMEM((ny, rows, lanes), BF16),
            pltpu.VMEM((2, rows, WIDTH), BF16),
            pltpu.VMEM((nz, rows, WIDTH), BF16),
            pltpu.VMEM((ny, rows, lanes), BF16),
            pltpu.VMEM((WIDTH, lanes), BF16),
        ]

    results = (
        ((length, WIDTH), BF16),
        ((length, WIDTH), F32),
        ((length, WIDTH), F32),
        ((length, WIDTH), BF16),
        ((depth, WIDTH), F32),
    )
    near, far = 2 * NEAR, nz - 2 * NEAR - 1
    vmem = pl.BlockSpec(memory_space=pltpu.VMEM)
    anywhere = pl.BlockSpec(memory_space=pl.ANY)
    held = pl.pallas_call(
        functools.partial(kernel, nz, ny, nt),
        out_shape=tuple(pltpu.VMEM(shape, dtype) for shape, dtype in results),
        in_specs=[anywhere] * 9,
        out_specs=[vmem] * 5,
        scratch_shapes=[
            pltpu.VMEM(w.shape, BF16),
            pltpu.VMEM(v.shape, BF16),
            pltpu.VMEM(gf.shape, BF16),
            pltpu.VMEM(gb.shape, BF16),
            pltpu.VMEM(slack.shape, F32),
            pltpu.VMEM((2, 1, length), F32),
            pltpu.VMEM((1, WIDTH), F32),
            pltpu.VMEM(cot.shape, BF16),
            dma((9,)),
            pltpu.VMEM((nt, length, x.shape[1]), BF16),
            pltpu.VMEM((w.shape[0], length), BF16),
            pltpu.VMEM((ny, 1, lanes), F32),
            pltpu.VMEM((nz, 1, lanes), F32),
        ]
        + scan_buffers()
        + scan_buffers()
        + [
            pltpu.VMEM((far + 1, ny, depth, WIDTH), BF16),
            pltpu.VMEM((ny, far + 1, depth, WIDTH), BF16),
            pltpu.VMEM((far + 1, depth, WIDTH), BF16),
            pltpu.VMEM((far, depth, WIDTH), BF16),
            pltpu.VMEM((near, ny, depth, WIDTH), BF16),
            pltpu.VMEM((near, ny, depth, WIDTH), BF16),
            pltpu.VMEM((ny, depth, WIDTH), BF16),
            pltpu.VMEM((ny, depth, WIDTH), BF16),
            dma((len(EXCHANGES),)),
            dma((len(EXCHANGES) + nt // 2,)),
        ],
        compiler_params=pltpu.CompilerParams(collective_id=0, has_side_effects=True),
    )(x, w, v, gf, gb, slack, extra.transpose(0, 2, 1), scale.reshape(1, WIDTH), cot)
    return pl.pallas_call(
        store,
        out_shape=tuple(jax.ShapeDtypeStruct(shape, dtype) for shape, dtype in results),
        in_specs=[vmem] * 5,
        out_specs=[anywhere] * 5,
        scratch_shapes=[dma((5,))],
    )(*(in_vmem(a) for a in held))


def solution(mesh):
    torus = Mesh(mesh.devices.reshape(NZ, NY, mesh.shape["tp"]), ("sp_0", "sp_1", "tp"))
    sp = ("sp_0", "sp_1")
    return jax.shard_map(
        functools.partial(on_device, NZ, NY),
        mesh=torus,
        in_specs=(
            P(sp, "tp"),
            P(None, "tp"),
            P(sp, "tp"),
            P(sp, "tp"),
            P(sp, "tp"),
            P(None, "tp"),
            P(None, sp, "tp"),
            P("tp"),
            P(sp, "tp"),
        ),
        out_specs=(P(sp, "tp"),) * 5,
        check_vma=False,
    )
```

```python
import functools

import jax
import jax.numpy as jnp
from jax import lax
from jax.experimental import pallas as pl
from jax.experimental.pallas import tpu as pltpu
from jax.sharding import Mesh
from jax.sharding import PartitionSpec as P

WIDTH = 128
HALF = 128
NZ, NY = 12, 8
NEAR = 3
GROUPS = (2, 1)
EARLY, MIDDLE, LOW = 1, 3, 2
EPS = 1e-6
MESH_ID = pl.DeviceIdType.MESH
F32, BF16 = jnp.float32, jnp.bfloat16

NN = (((1,), (0,)), ((), ()))
NT = (((1,), (1,)), ((), ()))
TN = (((0,), (0,)), ((), ()))


def dot(a, b, dims):
    a, b = (p if isinstance(p, tuple) else (p,) for p in (a, b))
    total = lax.dot_general(a[0], b[0], dims, preferred_element_type=F32)
    for tail in a[1:]:
        total += lax.dot_general(tail, b[0], dims, preferred_element_type=F32)
    for tail in b[1:]:
        total += lax.dot_general(a[0], tail, dims, preferred_element_type=F32)
    return total


def pair_of(x):
    head = x.astype(BF16)
    return head, (x - head.astype(F32)).astype(BF16)


def cut(pair, *at):
    return tuple(part[at] for part in pair)


def pieces(x, count):
    parts = []
    for _ in range(count):
        part = x.astype(BF16)
        parts.append(part)
        x = x - part.astype(F32)
    return parts


def summed(triangle, x, count):
    return sum(dot(triangle, part, NN) for part in pieces(x, count))


def both(x):
    return jnp.concatenate([x, x], axis=1)


def swapped(x):
    return jnp.concatenate([x[:, WIDTH:], x[:, :WIDTH]], axis=1)


def remote(src, dst, send, recv, peer):
    return pltpu.make_async_remote_copy(
        src_ref=src, dst_ref=dst, send_sem=send, recv_sem=recv, device_id=peer, device_id_type=MESH_ID
    )


EXCHANGES = ("dy", "a1", "dz", "b1", "c1", "a2", "b2", "c2", "g0", "g1", "g2", "b3", "a4", "b4", "xo", "xf")


def kernel(
    nz, ny, nt,
    x_hbm, w_hbm, v_hbm, gf_hbm, gb_hbm, slack_hbm, extra_hbm, scale_hbm, cot_hbm,
    dq_ref, dgf_ref, dgb_ref, dv_ref, dw_ref,
    w_ref, v_ref, gf_ref, gb_ref, slack_ref, extra_ref, scale_ref, cot_ref, load_sem,
    xall, xturn, dec_y, dec_z,
    out1, in1, mid1, got1, back1, state1,
    out2, in2, mid2, got2, back2, state2,
    wa, wa_in, wa_mid, wa_got, wb, wb_in, wb_mid, wb_got,
    send_sem, recv_sem,
):
    z, y, t = lax.axis_index("sp_0"), lax.axis_index("sp_1"), lax.axis_index("tp")
    rows = WIDTH // ny
    length = v_ref.shape[0]
    width_in = xall.shape[2]

    def far_first(n):
        return sorted(range(1, n), key=lambda o: -min(o, n - o))

    def at_y(o):
        return lax.rem(y + o, ny)

    def at_z(o):
        return lax.rem(z + o, nz)

    partner = t + 1 - 2 * lax.rem(t, 2)
    steps = far_first(nt // 2)
    chips = [lax.rem(t + 2 * o, nt) for o in steps]

    loads = []
    for i, (src, dst) in enumerate(
        (
            (gf_hbm, gf_ref),
            (gb_hbm, gb_ref),
            (slack_hbm, slack_ref),
            (extra_hbm, extra_ref),
            (v_hbm, v_ref),
            (x_hbm, xall.at[t]),
            (w_hbm, w_ref),
            (cot_hbm, cot_ref),
            (scale_hbm, scale_ref),
        )
    ):
        load = pltpu.make_async_copy(src, dst, load_sem.at[i])
        load.start()
        loads.append(load)

    barrier = pltpu.get_barrier_semaphore()
    count = 0
    for o in far_first(nz):
        pl.semaphore_signal(barrier, inc=1, device_id={"sp_0": at_z(o)}, device_id_type=MESH_ID)
        count += 1
    for o in range(1, ny):
        pl.semaphore_signal(barrier, inc=1, device_id={"sp_1": at_y(o)}, device_id_type=MESH_ID)
        count += 1
    for k in [partner] + chips:
        pl.semaphore_signal(barrier, inc=1, device_id={"tp": k}, device_id_type=MESH_ID)
        count += 1

    def send(name, src, dst, peer, chip=None):
        n = EXCHANGES.index(name)
        m = n if chip is None else len(EXCHANGES) + chip
        remote(src, dst, send_sem.at[n], recv_sem.at[m], peer).start()

    def arrived(name, whole, peer, chip=None):
        n = EXCHANGES.index(name)
        m = n if chip is None else len(EXCHANGES) + chip
        remote(whole, whole, send_sem.at[n], recv_sem.at[m], peer).wait_recv()

    def gone(name, whole, peer):
        n = EXCHANGES.index(name)
        remote(whole, whole, send_sem.at[n], recv_sem.at[n], peer).wait_send()

    next_y, next_z = {"sp_1": at_y(1)}, {"sp_0": at_z(1)}
    others_y, others_z = pl.ds(0, ny - 1), pl.ds(0, nz - 1)

    for load in loads[:4]:
        load.wait()
    pre = jnp.concatenate([gf_ref[...], gb_ref[...]], axis=1).astype(F32)
    slack = jnp.concatenate([slack_ref[0:1, :], slack_ref[1:2, :]], axis=1)
    gate = jax.nn.sigmoid(-pre)
    key = slack * gate
    forget = jnp.log1p(-key)
    row_id = lax.broadcasted_iota(jnp.int32, (length, length), 0)
    col_id = lax.broadcasted_iota(jnp.int32, (length, length), 1)
    lower = row_id >= col_id
    upper = row_id <= col_id
    lower_ones = jnp.where(lower, 1.0, 0.0).astype(BF16)
    upper_ones = jnp.where(upper, 1.0, 0.0).astype(BF16)
    spikes_f = jnp.sum(jnp.where(lower, extra_ref[0], 0.0), axis=1, keepdims=True)
    spikes_b = jnp.sum(jnp.where(upper, extra_ref[1], 0.0), axis=1, keepdims=True)
    run = jnp.concatenate(
        [
            summed(lower_ones, forget[:, :WIDTH], 2) + spikes_f,
            summed(upper_ones, forget[:, WIDTH:], 2) + spikes_b,
        ],
        axis=1,
    )
    closing = jnp.concatenate([run[length - 1 :, :WIDTH], run[0:1, WIDTH:]], axis=1)
    to_end = jnp.exp(closing - run)
    key_end = (key * to_end).astype(BF16)
    loads[4].wait()
    v = v_ref[...]
    local = dot(v, key_end, TN)
    out1[...] = local.astype(BF16).reshape(ny, rows, 2 * WIDTH)
    dec_y[pl.ds(y, 1)] = closing[None]
    in1[pl.ds(y, 1)] = out1[pl.ds(y, 1)]

    pl.semaphore_wait(barrier, count)

    def first_phase(name, out, into):
        for o in far_first(ny):
            k = at_y(o)
            send(name, out.at[k], into.at[y], {"sp_1": k})

    def line_fold(into, decays):
        up, down = [None] * ny, [None] * ny
        total = jnp.zeros((rows, WIDTH), F32)
        for k in range(ny):
            up[k] = total
            total = jnp.exp(decays[k][:, :WIDTH]) * total + into[k, :, :WIDTH].astype(F32)
        total_up = total
        total = jnp.zeros((rows, WIDTH), F32)
        for k in reversed(range(ny)):
            down[k] = total
            total = jnp.exp(decays[k][:, WIDTH:]) * total + into[k, :, WIDTH:].astype(F32)
        return up, down, total_up, total

    def second_phase(name, mid, got, totals):
        mid[0] = totals[0].astype(BF16)
        mid[1] = totals[1].astype(BF16)
        got[pl.ds(z, 1)] = jnp.zeros((1, rows, WIDTH), BF16)
        for o in far_first(nz):
            k = at_z(o)
            side = jnp.where(k > z, 0, 1)
            send(name, mid.at[side], got.at[z], {"sp_0": k})

    def line_entry(got, decays):
        above = jnp.zeros((rows, WIDTH), F32)
        for k in range(nz):
            new = jnp.exp(decays[k][:, :WIDTH]) * above + got[k].astype(F32)
            above = jnp.where(k < z, new, above)
        below = jnp.zeros((rows, WIDTH), F32)
        for k in reversed(range(nz)):
            new = jnp.exp(decays[k][:, WIDTH:]) * below + got[k].astype(F32)
            below = jnp.where(k > z, new, below)
        return above, below

    def third_phase(name, back, state, entry, prefixes, decays):
        above, below = entry
        up, down = prefixes
        past = jnp.zeros((1, WIDTH), F32)
        first = []
        for k in range(ny):
            first.append(jnp.exp(past) * above + up[k])
            past = past + decays[k][:, :WIDTH]
        past = jnp.zeros((1, WIDTH), F32)
        second = [None] * ny
        for k in reversed(range(ny)):
            second[k] = jnp.exp(past) * below + down[k]
            past = past + decays[k][:, WIDTH:]
        for k in range(ny):
            back[k] = jnp.concatenate([first[k], second[k]], axis=1).astype(BF16)
        here = pl.ds(pl.multiple_of(y * rows, rows), rows)
        for o in far_first(ny):
            k = at_y(o)
            send(name, back.at[k], state.at[here, :], {"sp_1": k})
        state[here, :] = back[pl.ds(y, 1)].reshape(rows, 2 * WIDTH)

    for o in far_first(ny):
        send("dy", dec_y.at[y], dec_y.at[y], {"sp_1": at_y(o)})
    first_phase("a1", out1, in1)
    loads[5].wait()
    for i, k in enumerate(chips):
        send("xo", xall.at[t], xall.at[t], {"tp": k}, i)
    send("xo", xall.at[t], xall.at[t], {"tp": partner}, len(chips))

    first_half = lax.broadcasted_iota(jnp.int32, (length, 2 * WIDTH), 0) < HALF
    centre = [run[HALF // 2 - 1 : HALF // 2], run[HALF + HALF // 2 - 1 : HALF + HALF // 2]]
    middle = jnp.where(first_half, centre[0], centre[1])
    grow = jnp.exp(run - middle)
    shrink = jnp.exp(middle - run)
    from_start = jnp.exp(run)
    keys = pair_of(key * shrink)
    step_f = jnp.exp(centre[1][:, :WIDTH] - centre[0][:, :WIDTH])
    step_b = jnp.exp(centre[0][:, WIDTH:] - centre[1][:, WIDTH:])

    arrived("dy", dec_y.at[others_y], next_y)
    decays1 = [dec_y[k] for k in range(ny)]
    line_total = sum(decays1[1:], decays1[0])
    dec_z[pl.ds(z, 1)] = line_total[None]
    for o in far_first(nz):
        send("dz", dec_z.at[z], dec_z.at[z], {"sp_0": at_z(o)})
    arrived("a1", in1.at[others_y], next_y)
    up, down, total_up, total_down = line_fold(in1, decays1)
    second_phase("b1", mid1, got1, (total_up, total_down))

    arrived("dz", dec_z.at[others_z], next_z)
    arrived("b1", got1.at[others_z], next_z)
    lines1 = [dec_z[k] for k in range(nz)]
    entry = line_entry(got1, lines1)
    third_phase("c1", back1, state1, entry, (up, down), decays1)

    for o, k in zip(steps, chips):
        arrived("xo", xall.at[k], {"tp": k}, steps.index(nt // 2 - o))
        send("xf", xall.at[k], xall.at[k], {"tp": partner})
    arrived("xo", xall.at[partner], {"tp": partner}, len(chips))
    if chips:
        arrived("xf", xall.at[pl.ds(0, len(chips))], {"tp": partner})
    for load in loads[6:]:
        load.wait()
    raw = jnp.zeros((length, WIDTH), F32)
    for k in range(nt):
        raw += dot(xall[k], w_ref[pl.ds(k * width_in, width_in), :], NN)
    raw = raw.astype(BF16).astype(F32)
    sig = jax.nn.sigmoid(raw)
    root = WIDTH**-0.5
    query = both(raw * sig * root)
    queries = query * grow
    query_in = pair_of(query * from_start)

    lo, hi = slice(0, HALF), slice(HALF, 2 * HALF)
    fw, bw = slice(0, WIDTH), slice(WIDTH, 2 * WIDTH)
    far_f = pair_of(queries[hi, fw] * step_f)
    far_b = pair_of(queries[lo, bw] * step_b)
    queries = pair_of(queries)
    low = lower[lo, lo]
    upp = upper[lo, lo]

    def near(a):
        return jnp.where(low, dot(cut(queries, a, fw), cut(keys, a, fw), NT), 0.0) + jnp.where(
            upp, dot(cut(queries, a, bw), cut(keys, a, bw), NT), 0.0
        )

    scores = jnp.concatenate(
        [
            jnp.concatenate([near(lo), dot(far_b, cut(keys, hi, bw), NT)], axis=1),
            jnp.concatenate([dot(far_f, cut(keys, lo, fw), NT), near(hi)], axis=1),
        ],
        axis=0,
    )
    scores = pair_of(scores)
    inside = dot(scores, v, NN)
    for k in range(nt):
        xturn[pl.ds(k * width_in, width_in), :] = xall[k].T

    arrived("c1", state1.at[pl.ds(0, WIDTH - rows), :], next_y)
    state = state1[...]
    mixed = inside + dot(query_in, state, NT)
    inv = lax.rsqrt(jnp.mean(mixed * mixed, axis=1, keepdims=True) + EPS)
    weighted = cot_ref[...].astype(F32) * scale_ref[...]
    along = jnp.mean(weighted * mixed, axis=1, keepdims=True)
    grad_out = pair_of(inv * (weighted - mixed * (inv * inv * along)))

    sense = dot(grad_out, query_in, TN)
    out2[...] = swapped(sense).astype(BF16).reshape(ny, rows, 2 * WIDTH)
    in2[pl.ds(y, 1)] = out2[pl.ds(y, 1)]
    first_phase("a2", out2, in2)

    cross = dot(grad_out, v, NT)
    cross_low = [pair_of(jnp.where(low, cross[a, a], 0.0)) for a in (lo, hi)]
    cross_upp = [pair_of(jnp.where(upp, cross[a, a], 0.0)) for a in (lo, hi)]
    cross_f, cross_b = pair_of(cross[hi, lo]), pair_of(cross[lo, hi])
    dq_f = jnp.concatenate(
        [
            dot(cross_low[0], cut(keys, lo, fw), NN),
            dot(cross_low[1], cut(keys, hi, fw), NN) + step_f * dot(cross_f, cut(keys, lo, fw), NN),
        ],
        axis=0,
    )
    dq_b = jnp.concatenate(
        [
            dot(cross_upp[0], cut(keys, lo, bw), NN) + step_b * dot(cross_b, cut(keys, hi, bw), NN),
            dot(cross_upp[1], cut(keys, hi, bw), NN),
        ],
        axis=0,
    )
    dq = grow * jnp.concatenate([dq_f, dq_b], axis=1) + from_start * dot(grad_out, state, NN)
    draw = (dq[:, fw] + dq[:, bw]) * (root * sig * (1.0 + raw * (1.0 - sig)))
    draw = draw.astype(BF16)
    dq_ref[...] = draw

    part = ny * wa.shape[2]
    far, near = nz - 2 * NEAR - 1, 2 * NEAR
    far_turn = sum(jnp.where(z + NEAR + 1 + i < nz, 1, 0) for i in range(far))
    near_at = [i + 1 + (nz - 1 - 2 * NEAR) * (i // NEAR) for i in range(near)]
    near_turn = sum(jnp.where(z + o < nz, 1, 0) for o in near_at)
    first, second = GROUPS
    slots = [*range(first + second), None, *range(first + second, far)]
    groups = [slice(0, first), slice(first, first + second + 1), slice(first + second + 1, far + 1)]

    def far_index(rank):
        return lax.rem(far_turn + rank, far)

    def far_owner(index):
        return lax.rem(z + NEAR + 1 + index, nz)

    def terms(owner):
        start = pl.multiple_of(owner * part, part)
        return dot(xturn[pl.ds(start, part), :], draw, NN).astype(BF16).reshape(wa.shape[1:])

    def far_send(g):
        for o in far_first(ny):
            k = at_y(o)
            send(f"g{g}", wa.at[groups[g], k], wa_in.at[y, groups[g]], {"sp_1": k})

    def far_pass(g):
        arrived(f"g{g}", wa_in.at[others_y, groups[g]], next_y)
        count = groups[g].stop - groups[g].start
        acc = wa[groups[g], pl.ds(y, 1)].astype(F32).reshape(count, *wa_mid.shape[1:])
        for o in range(1, ny):
            acc += wa_in[pl.ds(at_y(o), 1), groups[g]].astype(F32).reshape(acc.shape)
        wa_mid[groups[g]] = acc.astype(BF16)
        kept = None
        for n, rank in enumerate(slots[groups[g]]):
            slot = groups[g].start + n
            if rank is None:
                kept = acc[n]
            else:
                i = far_index(rank)
                send("b4", wa_mid.at[slot], wa_got.at[i], {"sp_0": far_owner(i)})
        return kept

    def fill(g):
        for slot in range(groups[g].start, groups[g].stop):
            wa[slot] = terms(z if slots[slot] is None else far_owner(far_index(slots[slot])))

    def near_send(ranks):
        for rank in ranks:
            i = lax.rem(near_turn + rank, near)
            o = i + 1 + (nz - 1 - 2 * NEAR) * (i // NEAR)
            send("b3", wb.at[i], wb_in.at[i], {"sp_0": lax.rem(z + o, nz)})

    def near_fill(ranks):
        for rank in ranks:
            i = lax.rem(near_turn + rank, near)
            o = i + 1 + (nz - 1 - 2 * NEAR) * (i // NEAR)
            wb[pl.ds(i, 1)] = terms(lax.rem(z + o, nz))[None]

    fill(0)
    far_send(0)
    near_fill(range(EARLY + 1))
    near_send(range(EARLY))

    @pl.when(z < LOW)
    def _():
        near_send(range(EARLY, EARLY + 1))

    fill(1)
    far_send(1)
    fill(2)
    far_send(2)
    near_fill(range(EARLY + 1, near))

    decays2 = [swapped(d) for d in decays1]
    lines2 = [swapped(d) for d in lines1]
    arrived("a2", in2.at[others_y], next_y)
    up, down, total_up, total_down = line_fold(in2, decays2)
    second_phase("b2", mid2, got2, (total_up, total_down))
    @pl.when(z >= LOW)
    def _():
        near_send(range(EARLY, EARLY + 1))

    near_send(range(EARLY + 1, MIDDLE))

    @pl.when(z < LOW)
    def _():
        near_send(range(MIDDLE, near))

    dv = dot(scores, grad_out, TN)
    dk_f = jnp.concatenate(
        [
            dot(cross_low[0], cut(queries, lo, fw), TN) + dot(cross_f, far_f, TN),
            dot(cross_low[1], cut(queries, hi, fw), TN),
        ],
        axis=0,
    )
    dk_b = jnp.concatenate(
        [
            dot(cross_upp[0], cut(queries, lo, bw), TN),
            dot(cross_upp[1], cut(queries, hi, bw), TN) + dot(cross_b, far_b, TN),
        ],
        axis=0,
    )
    dk = shrink * jnp.concatenate([dk_f, dk_b], axis=1)
    drift = query * dq - key * dk
    left = jnp.exp(closing) * state.astype(F32) + local

    far_pass(0)

    @pl.when(z >= LOW)
    def _():
        near_send(range(MIDDLE, near))

    arrived("b2", got2.at[others_z], next_z)
    entry = line_entry(got2, lines2)
    third_phase("c2", back2, state2, entry, (up, down), decays2)

    own = far_pass(1)
    far_pass(2)
    arrived("b3", wb_in, next_z)
    acc = wb_in[0].astype(F32)
    for i in range(1, near):
        acc += wb_in[i].astype(F32)
    wb_mid[...] = acc.astype(BF16)
    for o in far_first(ny):
        k = at_y(o)
        send("a4", wb_mid.at[k], wb_got.at[y], {"sp_1": k})
    own += wb_mid[pl.ds(y, 1)].astype(F32).reshape(dw_ref.shape)

    arrived("c2", state2.at[pl.ds(0, WIDTH - rows), :], next_y)
    after = swapped(state2[...])
    dv_ref[...] = (dv + dot(key_end, after, NT)).astype(BF16)
    dk_end = to_end * dot(v, after, NN)
    ends = jnp.sum(after.astype(F32) * left, axis=0, keepdims=True)
    drift = drift - key * dk_end
    drift = jnp.concatenate(
        [summed(upper_ones, drift[:, fw], 2), summed(lower_ones, drift[:, bw], 2)], axis=1
    )
    dkey = dk + dk_end - (drift + ends) / (1.0 - key)
    dgate = -key * (1.0 - gate) * dkey
    dgf_ref[...] = dgate[:, fw]
    dgb_ref[...] = dgate[:, bw]

    arrived("a4", wb_got.at[others_y], next_y)
    for o in range(1, ny):
        own += wb_got[pl.ds(at_y(o), 1)].astype(F32).reshape(own.shape)
    arrived("b4", wa_got, next_z)
    for i in range(far):
        own += wa_got[i].astype(F32)
    dw_ref[...] = own

    for name, whole in (
        ("dy", dec_y.at[others_y]),
        ("a1", out1.at[others_y]),
        ("c1", back1.at[others_y]),
        ("a2", out2.at[others_y]),
        ("c2", back2.at[others_y]),
        ("g0", wa_in.at[others_y, groups[0]]),
        ("g1", wa_in.at[others_y, groups[1]]),
        ("g2", wa_in.at[others_y, groups[2]]),
        ("a4", wb_got.at[others_y]),
    ):
        gone(name, whole, next_y)
    for name, whole in (
        ("dz", dec_z.at[others_z]),
        ("b1", got1.at[others_z]),
        ("b2", got2.at[others_z]),
        ("b3", wb_in),
        ("b4", wa_got),
    ):
        gone(name, whole, next_z)
    gone("xo", xall.at[pl.ds(0, len(chips) + 1)], {"tp": partner})
    if chips:
        gone("xf", xall.at[pl.ds(0, len(chips))], {"tp": partner})


def store(*refs):
    sources, targets, sems = refs[:5], refs[5:10], refs[10]
    copies = [
        pltpu.make_async_copy(src, dst, sems.at[i])
        for i, (src, dst) in enumerate(zip(sources, targets))
    ]
    for copy in copies:
        copy.start()
    for copy in copies:
        copy.wait()


def in_vmem(a):
    return pltpu.with_memory_space_constraint(a, pltpu.VMEM)


def on_device(nz, ny, x, w, v, gf, gb, slack, extra, scale, cot):
    nt = w.shape[0] // x.shape[1]
    length = v.shape[0]
    rows = WIDTH // ny
    depth = w.shape[0] // (nz * ny)
    lanes = 2 * WIDTH
    dma = pltpu.SemaphoreType.DMA

    def scan_buffers():
        return [
            pltpu.VMEM((ny, rows, lanes), BF16),
            pltpu.VMEM((ny, rows, lanes), BF16),
            pltpu.VMEM((2, rows, WIDTH), BF16),
            pltpu.VMEM((nz, rows, WIDTH), BF16),
            pltpu.VMEM((ny, rows, lanes), BF16),
            pltpu.VMEM((WIDTH, lanes), BF16),
        ]

    results = (
        ((length, WIDTH), BF16),
        ((length, WIDTH), F32),
        ((length, WIDTH), F32),
        ((length, WIDTH), BF16),
        ((depth, WIDTH), F32),
    )
    near, far = 2 * NEAR, nz - 2 * NEAR - 1
    vmem = pl.BlockSpec(memory_space=pltpu.VMEM)
    anywhere = pl.BlockSpec(memory_space=pl.ANY)
    held = pl.pallas_call(
        functools.partial(kernel, nz, ny, nt),
        out_shape=tuple(pltpu.VMEM(shape, dtype) for shape, dtype in results),
        in_specs=[anywhere] * 9,
        out_specs=[vmem] * 5,
        scratch_shapes=[
            pltpu.VMEM(w.shape, BF16),
            pltpu.VMEM(v.shape, BF16),
            pltpu.VMEM(gf.shape, BF16),
            pltpu.VMEM(gb.shape, BF16),
            pltpu.VMEM(slack.shape, F32),
            pltpu.VMEM((2, 1, length), F32),
            pltpu.VMEM((1, WIDTH), F32),
            pltpu.VMEM(cot.shape, BF16),
            dma((9,)),
            pltpu.VMEM((nt, length, x.shape[1]), BF16),
            pltpu.VMEM((w.shape[0], length), BF16),
            pltpu.VMEM((ny, 1, lanes), F32),
            pltpu.VMEM((nz, 1, lanes), F32),
        ]
        + scan_buffers()
        + scan_buffers()
        + [
            pltpu.VMEM((far + 1, ny, depth, WIDTH), BF16),
            pltpu.VMEM((ny, far + 1, depth, WIDTH), BF16),
            pltpu.VMEM((far + 1, depth, WIDTH), BF16),
            pltpu.VMEM((far, depth, WIDTH), BF16),
            pltpu.VMEM((near, ny, depth, WIDTH), BF16),
            pltpu.VMEM((near, ny, depth, WIDTH), BF16),
            pltpu.VMEM((ny, depth, WIDTH), BF16),
            pltpu.VMEM((ny, depth, WIDTH), BF16),
            dma((len(EXCHANGES),)),
            dma((len(EXCHANGES) + nt // 2,)),
        ],
        compiler_params=pltpu.CompilerParams(collective_id=0, has_side_effects=True),
    )(x, w, v, gf, gb, slack, extra.transpose(0, 2, 1), scale.reshape(1, WIDTH), cot)
    return pl.pallas_call(
        store,
        out_shape=tuple(jax.ShapeDtypeStruct(shape, dtype) for shape, dtype in results),
        in_specs=[vmem] * 5,
        out_specs=[anywhere] * 5,
        scratch_shapes=[dma((5,))],
    )(*(in_vmem(a) for a in held))


def solution(mesh):
    torus = Mesh(mesh.devices.reshape(NZ, NY, mesh.shape["tp"]), ("sp_0", "sp_1", "tp"))
    sp = ("sp_0", "sp_1")
    return jax.shard_map(
        functools.partial(on_device, NZ, NY),
        mesh=torus,
        in_specs=(
            P(sp, "tp"),
            P(None, "tp"),
            P(sp, "tp"),
            P(sp, "tp"),
            P(sp, "tp"),
            P(None, "tp"),
            P(None, sp, "tp"),
            P("tp"),
            P(sp, "tp"),
        ),
        out_specs=(P(sp, "tp"),) * 5,
        check_vma=False,
    )
```

```python
import functools

import jax
import jax.numpy as jnp
from jax import lax
from jax.experimental import pallas as pl
from jax.experimental.pallas import tpu as pltpu
from jax.sharding import Mesh
from jax.sharding import PartitionSpec as P

WIDTH = 128
HALF = 128
NZ, NY = 12, 8
NEAR = 3
GROUPS = (2, 1)
EARLY, MIDDLE, LOW = 1, 3, 2
EPS = 1e-6
MESH_ID = pl.DeviceIdType.MESH
F32, BF16 = jnp.float32, jnp.bfloat16

NN = (((1,), (0,)), ((), ()))
NT = (((1,), (1,)), ((), ()))
TN = (((0,), (0,)), ((), ()))


def dot(a, b, dims):
    a, b = (p if isinstance(p, tuple) else (p,) for p in (a, b))
    total = lax.dot_general(a[0], b[0], dims, preferred_element_type=F32)
    for tail in a[1:]:
        total += lax.dot_general(tail, b[0], dims, preferred_element_type=F32)
    for tail in b[1:]:
        total += lax.dot_general(a[0], tail, dims, preferred_element_type=F32)
    return total


def pair_of(x):
    head = x.astype(BF16)
    return head, (x - head.astype(F32)).astype(BF16)


def cut(pair, *at):
    return tuple(part[at] for part in pair)


def pieces(x, count):
    parts = []
    for _ in range(count):
        part = x.astype(BF16)
        parts.append(part)
        x = x - part.astype(F32)
    return parts


def summed(triangle, x, count):
    return sum(dot(triangle, part, NN) for part in pieces(x, count))


def both(x):
    return jnp.concatenate([x, x], axis=1)


def swapped(x):
    return jnp.concatenate([x[:, WIDTH:], x[:, :WIDTH]], axis=1)


def remote(src, dst, send, recv, peer):
    return pltpu.make_async_remote_copy(
        src_ref=src, dst_ref=dst, send_sem=send, recv_sem=recv, device_id=peer, device_id_type=MESH_ID
    )


EXCHANGES = ("dy", "a1", "dz", "b1", "c1", "a2", "b2", "c2", "g0", "g1", "g2", "b3", "a4", "b4", "xo", "xf")


def kernel(
    nz, ny, nt,
    x_hbm, w_hbm, v_hbm, gf_hbm, gb_hbm, slack_hbm, extra_hbm, scale_hbm, cot_hbm,
    dq_ref, dgf_ref, dgb_ref, dv_ref, dw_ref,
    w_ref, v_ref, gf_ref, gb_ref, slack_ref, extra_ref, scale_ref, cot_ref, load_sem,
    xall, xturn, dec_y, dec_z,
    out1, in1, mid1, got1, back1, state1,
    out2, in2, mid2, got2, back2, state2,
    wa, wa_in, wa_mid, wa_got, wb, wb_in, wb_mid, wb_got,
    send_sem, recv_sem,
):
    z, y, t = lax.axis_index("sp_0"), lax.axis_index("sp_1"), lax.axis_index("tp")
    rows = WIDTH // ny
    length = v_ref.shape[0]
    width_in = xall.shape[2]

    def far_first(n):
        return sorted(range(1, n), key=lambda o: -min(o, n - o))

    def at_y(o):
        return lax.rem(y + o, ny)

    def at_z(o):
        return lax.rem(z + o, nz)

    partner = t + 1 - 2 * lax.rem(t, 2)
    steps = far_first(nt // 2)
    chips = [lax.rem(t + 2 * o, nt) for o in steps]

    loads = []
    for i, (src, dst) in enumerate(
        (
            (gf_hbm, gf_ref),
            (gb_hbm, gb_ref),
            (slack_hbm, slack_ref),
            (extra_hbm, extra_ref),
            (v_hbm, v_ref),
            (x_hbm, xall.at[t]),
            (w_hbm, w_ref),
            (cot_hbm, cot_ref),
            (scale_hbm, scale_ref),
        )
    ):
        load = pltpu.make_async_copy(src, dst, load_sem.at[i])
        load.start()
        loads.append(load)

    barrier = pltpu.get_barrier_semaphore()
    count = 0
    for o in far_first(nz):
        pl.semaphore_signal(barrier, inc=1, device_id={"sp_0": at_z(o)}, device_id_type=MESH_ID)
        count += 1
    for o in range(1, ny):
        pl.semaphore_signal(barrier, inc=1, device_id={"sp_1": at_y(o)}, device_id_type=MESH_ID)
        count += 1
    for k in [partner] + chips:
        pl.semaphore_signal(barrier, inc=1, device_id={"tp": k}, device_id_type=MESH_ID)
        count += 1

    def send(name, src, dst, peer, chip=None):
        n = EXCHANGES.index(name)
        m = n if chip is None else len(EXCHANGES) + chip
        remote(src, dst, send_sem.at[n], recv_sem.at[m], peer).start()

    def arrived(name, whole, peer, chip=None):
        n = EXCHANGES.index(name)
        m = n if chip is None else len(EXCHANGES) + chip
        remote(whole, whole, send_sem.at[n], recv_sem.at[m], peer).wait_recv()

    def gone(name, whole, peer):
        n = EXCHANGES.index(name)
        remote(whole, whole, send_sem.at[n], recv_sem.at[n], peer).wait_send()

    next_y, next_z = {"sp_1": at_y(1)}, {"sp_0": at_z(1)}
    others_y, others_z = pl.ds(0, ny - 1), pl.ds(0, nz - 1)

    for load in loads[:4]:
        load.wait()
    pre = jnp.concatenate([gf_ref[...], gb_ref[...]], axis=1).astype(F32)
    slack = jnp.concatenate([slack_ref[0:1, :], slack_ref[1:2, :]], axis=1)
    gate = jax.nn.sigmoid(-pre)
    key = slack * gate
    forget = jnp.log1p(-key)
    row_id = lax.broadcasted_iota(jnp.int32, (length, length), 0)
    col_id = lax.broadcasted_iota(jnp.int32, (length, length), 1)
    lower = row_id >= col_id
    upper = row_id <= col_id
    lower_ones = jnp.where(lower, 1.0, 0.0).astype(BF16)
    upper_ones = jnp.where(upper, 1.0, 0.0).astype(BF16)
    spikes_f = jnp.sum(jnp.where(lower, extra_ref[0], 0.0), axis=1, keepdims=True)
    spikes_b = jnp.sum(jnp.where(upper, extra_ref[1], 0.0), axis=1, keepdims=True)
    run = jnp.concatenate(
        [
            summed(lower_ones, forget[:, :WIDTH], 2) + spikes_f,
            summed(upper_ones, forget[:, WIDTH:], 2) + spikes_b,
        ],
        axis=1,
    )
    closing = jnp.concatenate([run[length - 1 :, :WIDTH], run[0:1, WIDTH:]], axis=1)
    to_end = jnp.exp(closing - run)
    key_end = (key * to_end).astype(BF16)
    loads[4].wait()
    v = v_ref[...]
    local = dot(v, key_end, TN)
    out1[...] = local.astype(BF16).reshape(ny, rows, 2 * WIDTH)
    dec_y[pl.ds(y, 1)] = closing[None]
    in1[pl.ds(y, 1)] = out1[pl.ds(y, 1)]

    pl.semaphore_wait(barrier, count)

    def first_phase(name, out, into):
        for o in far_first(ny):
            k = at_y(o)
            send(name, out.at[k], into.at[y], {"sp_1": k})

    def line_fold(into, decays):
        up, down = [None] * ny, [None] * ny
        total = jnp.zeros((rows, WIDTH), F32)
        for k in range(ny):
            up[k] = total
            total = jnp.exp(decays[k][:, :WIDTH]) * total + into[k, :, :WIDTH].astype(F32)
        total_up = total
        total = jnp.zeros((rows, WIDTH), F32)
        for k in reversed(range(ny)):
            down[k] = total
            total = jnp.exp(decays[k][:, WIDTH:]) * total + into[k, :, WIDTH:].astype(F32)
        return up, down, total_up, total

    def second_phase(name, mid, got, totals):
        mid[0] = totals[0].astype(BF16)
        mid[1] = totals[1].astype(BF16)
        got[pl.ds(z, 1)] = jnp.zeros((1, rows, WIDTH), BF16)
        for o in far_first(nz):
            k = at_z(o)
            side = jnp.where(k > z, 0, 1)
            send(name, mid.at[side], got.at[z], {"sp_0": k})

    def line_entry(got, decays):
        above = jnp.zeros((rows, WIDTH), F32)
        for k in range(nz):
            new = jnp.exp(decays[k][:, :WIDTH]) * above + got[k].astype(F32)
            above = jnp.where(k < z, new, above)
        below = jnp.zeros((rows, WIDTH), F32)
        for k in reversed(range(nz)):
            new = jnp.exp(decays[k][:, WIDTH:]) * below + got[k].astype(F32)
            below = jnp.where(k > z, new, below)
        return above, below

    def third_phase(name, back, state, entry, prefixes, decays):
        above, below = entry
        up, down = prefixes
        past = jnp.zeros((1, WIDTH), F32)
        first = []
        for k in range(ny):
            first.append(jnp.exp(past) * above + up[k])
            past = past + decays[k][:, :WIDTH]
        past = jnp.zeros((1, WIDTH), F32)
        second = [None] * ny
        for k in reversed(range(ny)):
            second[k] = jnp.exp(past) * below + down[k]
            past = past + decays[k][:, WIDTH:]
        for k in range(ny):
            back[k] = jnp.concatenate([first[k], second[k]], axis=1).astype(BF16)
        here = pl.ds(pl.multiple_of(y * rows, rows), rows)
        for o in far_first(ny):
            k = at_y(o)
            send(name, back.at[k], state.at[here, :], {"sp_1": k})
        state[here, :] = back[pl.ds(y, 1)].reshape(rows, 2 * WIDTH)

    for o in far_first(ny):
        send("dy", dec_y.at[y], dec_y.at[y], {"sp_1": at_y(o)})
    first_phase("a1", out1, in1)
    loads[5].wait()
    for i, k in enumerate(chips):
        send("xo", xall.at[t], xall.at[t], {"tp": k}, i)
    send("xo", xall.at[t], xall.at[t], {"tp": partner}, len(chips))

    first_half = lax.broadcasted_iota(jnp.int32, (length, 2 * WIDTH), 0) < HALF
    centre = [run[HALF // 2 - 1 : HALF // 2], run[HALF + HALF // 2 - 1 : HALF + HALF // 2]]
    middle = jnp.where(first_half, centre[0], centre[1])
    grow = jnp.exp(run - middle)
    shrink = jnp.exp(middle - run)
    from_start = jnp.exp(run)
    keys = pair_of(key * shrink)
    step_f = jnp.exp(centre[1][:, :WIDTH] - centre[0][:, :WIDTH])
    step_b = jnp.exp(centre[0][:, WIDTH:] - centre[1][:, WIDTH:])

    arrived("dy", dec_y.at[others_y], next_y)
    decays1 = [dec_y[k] for k in range(ny)]
    line_total = sum(decays1[1:], decays1[0])
    dec_z[pl.ds(z, 1)] = line_total[None]
    for o in far_first(nz):
        send("dz", dec_z.at[z], dec_z.at[z], {"sp_0": at_z(o)})
    arrived("a1", in1.at[others_y], next_y)
    up, down, total_up, total_down = line_fold(in1, decays1)
    second_phase("b1", mid1, got1, (total_up, total_down))

    arrived("dz", dec_z.at[others_z], next_z)
    arrived("b1", got1.at[others_z], next_z)
    lines1 = [dec_z[k] for k in range(nz)]
    entry = line_entry(got1, lines1)
    third_phase("c1", back1, state1, entry, (up, down), decays1)

    for o, k in zip(steps, chips):
        arrived("xo", xall.at[k], {"tp": k}, steps.index(nt // 2 - o))
        send("xf", xall.at[k], xall.at[k], {"tp": partner})
    arrived("xo", xall.at[partner], {"tp": partner}, len(chips))
    if chips:
        arrived("xf", xall.at[pl.ds(0, len(chips))], {"tp": partner})
    for load in loads[6:]:
        load.wait()
    raw = jnp.zeros((length, WIDTH), F32)
    for k in range(nt):
        raw += dot(xall[k], w_ref[pl.ds(k * width_in, width_in), :], NN)
    raw = raw.astype(BF16).astype(F32)
    sig = jax.nn.sigmoid(raw)
    root = WIDTH**-0.5
    query = both(raw * sig * root)
    queries = query * grow
    query_in = pair_of(query * from_start)

    lo, hi = slice(0, HALF), slice(HALF, 2 * HALF)
    fw, bw = slice(0, WIDTH), slice(WIDTH, 2 * WIDTH)
    far_f = pair_of(queries[hi, fw] * step_f)
    far_b = pair_of(queries[lo, bw] * step_b)
    queries = pair_of(queries)
    low = lower[lo, lo]
    upp = upper[lo, lo]

    def near(a):
        return jnp.where(low, dot(cut(queries, a, fw), cut(keys, a, fw), NT), 0.0) + jnp.where(
            upp, dot(cut(queries, a, bw), cut(keys, a, bw), NT), 0.0
        )

    scores = jnp.concatenate(
        [
            jnp.concatenate([near(lo), dot(far_b, cut(keys, hi, bw), NT)], axis=1),
            jnp.concatenate([dot(far_f, cut(keys, lo, fw), NT), near(hi)], axis=1),
        ],
        axis=0,
    )
    scores = pair_of(scores)
    inside = dot(scores, v, NN)
    for k in range(nt):
        xturn[pl.ds(k * width_in, width_in), :] = xall[k].T

    arrived("c1", state1.at[pl.ds(0, WIDTH - rows), :], next_y)
    state = state1[...]
    mixed = inside + dot(query_in, state, NT)
    inv = lax.rsqrt(jnp.mean(mixed * mixed, axis=1, keepdims=True) + EPS)
    weighted = cot_ref[...].astype(F32) * scale_ref[...]
    along = jnp.mean(weighted * mixed, axis=1, keepdims=True)
    grad_out = pair_of(inv * (weighted - mixed * (inv * inv * along)))

    sense = dot(grad_out, query_in, TN)
    out2[...] = swapped(sense).astype(BF16).reshape(ny, rows, 2 * WIDTH)
    in2[pl.ds(y, 1)] = out2[pl.ds(y, 1)]
    first_phase("a2", out2, in2)

    cross = dot(grad_out, v, NT)
    cross_low = [pair_of(jnp.where(low, cross[a, a], 0.0)) for a in (lo, hi)]
    cross_upp = [pair_of(jnp.where(upp, cross[a, a], 0.0)) for a in (lo, hi)]
    cross_f, cross_b = pair_of(cross[hi, lo]), pair_of(cross[lo, hi])
    dq_f = jnp.concatenate(
        [
            dot(cross_low[0], cut(keys, lo, fw), NN),
            dot(cross_low[1], cut(keys, hi, fw), NN) + step_f * dot(cross_f, cut(keys, lo, fw), NN),
        ],
        axis=0,
    )
    dq_b = jnp.concatenate(
        [
            dot(cross_upp[0], cut(keys, lo, bw), NN) + step_b * dot(cross_b, cut(keys, hi, bw), NN),
            dot(cross_upp[1], cut(keys, hi, bw), NN),
        ],
        axis=0,
    )
    dq = grow * jnp.concatenate([dq_f, dq_b], axis=1) + from_start * dot(grad_out, state, NN)
    draw = (dq[:, fw] + dq[:, bw]) * (root * sig * (1.0 + raw * (1.0 - sig)))
    draw = draw.astype(BF16)
    dq_ref[...] = draw

    part = ny * wa.shape[2]
    far, near = nz - 2 * NEAR - 1, 2 * NEAR
    far_turn = sum(jnp.where(z + NEAR + 1 + i < nz, 1, 0) for i in range(far))
    near_at = [i + 1 + (nz - 1 - 2 * NEAR) * (i // NEAR) for i in range(near)]
    near_turn = sum(jnp.where(z + o < nz, 1, 0) for o in near_at)
    first, second = GROUPS
    slots = [*range(first + second), None, *range(first + second, far)]
    groups = [slice(0, first), slice(first, first + second + 1), slice(first + second + 1, far + 1)]

    def far_index(rank):
        return lax.rem(far_turn + rank, far)

    def far_owner(index):
        return lax.rem(z + NEAR + 1 + index, nz)

    def terms(owner):
        start = pl.multiple_of(owner * part, part)
        return dot(xturn[pl.ds(start, part), :], draw, NN).astype(BF16).reshape(wa.shape[1:])

    def far_send(g):
        for o in far_first(ny):
            k = at_y(o)
            send(f"g{g}", wa.at[groups[g], k], wa_in.at[y, groups[g]], {"sp_1": k})

    def far_pass(g):
        arrived(f"g{g}", wa_in.at[others_y, groups[g]], next_y)
        count = groups[g].stop - groups[g].start
        acc = wa[groups[g], pl.ds(y, 1)].astype(F32).reshape(count, *wa_mid.shape[1:])
        for o in range(1, ny):
            acc += wa_in[pl.ds(at_y(o), 1), groups[g]].astype(F32).reshape(acc.shape)
        wa_mid[groups[g]] = acc.astype(BF16)
        kept = None
        for n, rank in enumerate(slots[groups[g]]):
            slot = groups[g].start + n
            if rank is None:
                kept = acc[n]
            else:
                i = far_index(rank)
                send("b4", wa_mid.at[slot], wa_got.at[i], {"sp_0": far_owner(i)})
        return kept

    def fill(g):
        for slot in range(groups[g].start, groups[g].stop):
            wa[slot] = terms(z if slots[slot] is None else far_owner(far_index(slots[slot])))

    def near_send(ranks):
        for rank in ranks:
            i = lax.rem(near_turn + rank, near)
            o = i + 1 + (nz - 1 - 2 * NEAR) * (i // NEAR)
            send("b3", wb.at[i], wb_in.at[i], {"sp_0": lax.rem(z + o, nz)})

    def near_fill(ranks):
        for rank in ranks:
            i = lax.rem(near_turn + rank, near)
            o = i + 1 + (nz - 1 - 2 * NEAR) * (i // NEAR)
            wb[pl.ds(i, 1)] = terms(lax.rem(z + o, nz))[None]

    fill(0)
    far_send(0)
    near_fill(range(EARLY + 1))
    near_send(range(EARLY))

    @pl.when(z < LOW)
    def _():
        near_send(range(EARLY, EARLY + 1))

    fill(1)
    far_send(1)
    fill(2)
    far_send(2)
    near_fill(range(EARLY + 1, near))

    decays2 = [swapped(d) for d in decays1]
    lines2 = [swapped(d) for d in lines1]
    arrived("a2", in2.at[others_y], next_y)
    up, down, total_up, total_down = line_fold(in2, decays2)
    second_phase("b2", mid2, got2, (total_up, total_down))
    @pl.when(z >= LOW)
    def _():
        near_send(range(EARLY, EARLY + 1))

    near_send(range(EARLY + 1, MIDDLE))

    @pl.when(z < LOW)
    def _():
        near_send(range(MIDDLE, near))

    dv = dot(scores, grad_out, TN)
    dk_f = jnp.concatenate(
        [
            dot(cross_low[0], cut(queries, lo, fw), TN) + dot(cross_f, far_f, TN),
            dot(cross_low[1], cut(queries, hi, fw), TN),
        ],
        axis=0,
    )
    dk_b = jnp.concatenate(
        [
            dot(cross_upp[0], cut(queries, lo, bw), TN),
            dot(cross_upp[1], cut(queries, hi, bw), TN) + dot(cross_b, far_b, TN),
        ],
        axis=0,
    )
    dk = shrink * jnp.concatenate([dk_f, dk_b], axis=1)
    drift = query * dq - key * dk
    left = jnp.exp(closing) * state.astype(F32) + local

    far_pass(0)

    @pl.when(z >= LOW)
    def _():
        near_send(range(MIDDLE, near))

    arrived("b2", got2.at[others_z], next_z)
    entry = line_entry(got2, lines2)
    third_phase("c2", back2, state2, entry, (up, down), decays2)

    def near_pass():
        arrived("b3", wb_in, next_z)
        acc = wb_in[0].astype(F32)
        for i in range(1, near):
            acc += wb_in[i].astype(F32)
        wb_mid[...] = acc.astype(BF16)
        for o in far_first(ny):
            k = at_y(o)
            send("a4", wb_mid.at[k], wb_got.at[y], {"sp_1": k})

    pl.when(z < LOW)(near_pass)
    own = far_pass(1)
    far_pass(2)
    pl.when(z >= LOW)(near_pass)
    own += wb_mid[pl.ds(y, 1)].astype(F32).reshape(dw_ref.shape)

    arrived("c2", state2.at[pl.ds(0, WIDTH - rows), :], next_y)
    after = swapped(state2[...])
    dv_ref[...] = (dv + dot(key_end, after, NT)).astype(BF16)
    dk_end = to_end * dot(v, after, NN)
    ends = jnp.sum(after.astype(F32) * left, axis=0, keepdims=True)
    drift = drift - key * dk_end
    drift = jnp.concatenate(
        [summed(upper_ones, drift[:, fw], 2), summed(lower_ones, drift[:, bw], 2)], axis=1
    )
    dkey = dk + dk_end - (drift + ends) / (1.0 - key)
    dgate = -key * (1.0 - gate) * dkey
    dgf_ref[...] = dgate[:, fw]
    dgb_ref[...] = dgate[:, bw]

    arrived("a4", wb_got.at[others_y], next_y)
    for o in range(1, ny):
        own += wb_got[pl.ds(at_y(o), 1)].astype(F32).reshape(own.shape)
    arrived("b4", wa_got, next_z)
    for i in range(far):
        own += wa_got[i].astype(F32)
    dw_ref[...] = own

    for name, whole in (
        ("dy", dec_y.at[others_y]),
        ("a1", out1.at[others_y]),
        ("c1", back1.at[others_y]),
        ("a2", out2.at[others_y]),
        ("c2", back2.at[others_y]),
        ("g0", wa_in.at[others_y, groups[0]]),
        ("g1", wa_in.at[others_y, groups[1]]),
        ("g2", wa_in.at[others_y, groups[2]]),
        ("a4", wb_got.at[others_y]),
    ):
        gone(name, whole, next_y)
    for name, whole in (
        ("dz", dec_z.at[others_z]),
        ("b1", got1.at[others_z]),
        ("b2", got2.at[others_z]),
        ("b3", wb_in),
        ("b4", wa_got),
    ):
        gone(name, whole, next_z)
    gone("xo", xall.at[pl.ds(0, len(chips) + 1)], {"tp": partner})
    if chips:
        gone("xf", xall.at[pl.ds(0, len(chips))], {"tp": partner})


def store(*refs):
    sources, targets, sems = refs[:5], refs[5:10], refs[10]
    copies = [
        pltpu.make_async_copy(src, dst, sems.at[i])
        for i, (src, dst) in enumerate(zip(sources, targets))
    ]
    for copy in copies:
        copy.start()
    for copy in copies:
        copy.wait()


def in_vmem(a):
    return pltpu.with_memory_space_constraint(a, pltpu.VMEM)


def on_device(nz, ny, x, w, v, gf, gb, slack, extra, scale, cot):
    nt = w.shape[0] // x.shape[1]
    length = v.shape[0]
    rows = WIDTH // ny
    depth = w.shape[0] // (nz * ny)
    lanes = 2 * WIDTH
    dma = pltpu.SemaphoreType.DMA

    def scan_buffers():
        return [
            pltpu.VMEM((ny, rows, lanes), BF16),
            pltpu.VMEM((ny, rows, lanes), BF16),
            pltpu.VMEM((2, rows, WIDTH), BF16),
            pltpu.VMEM((nz, rows, WIDTH), BF16),
            pltpu.VMEM((ny, rows, lanes), BF16),
            pltpu.VMEM((WIDTH, lanes), BF16),
        ]

    results = (
        ((length, WIDTH), BF16),
        ((length, WIDTH), F32),
        ((length, WIDTH), F32),
        ((length, WIDTH), BF16),
        ((depth, WIDTH), F32),
    )
    near, far = 2 * NEAR, nz - 2 * NEAR - 1
    vmem = pl.BlockSpec(memory_space=pltpu.VMEM)
    anywhere = pl.BlockSpec(memory_space=pl.ANY)
    held = pl.pallas_call(
        functools.partial(kernel, nz, ny, nt),
        out_shape=tuple(pltpu.VMEM(shape, dtype) for shape, dtype in results),
        in_specs=[anywhere] * 9,
        out_specs=[vmem] * 5,
        scratch_shapes=[
            pltpu.VMEM(w.shape, BF16),
            pltpu.VMEM(v.shape, BF16),
            pltpu.VMEM(gf.shape, BF16),
            pltpu.VMEM(gb.shape, BF16),
            pltpu.VMEM(slack.shape, F32),
            pltpu.VMEM((2, 1, length), F32),
            pltpu.VMEM((1, WIDTH), F32),
            pltpu.VMEM(cot.shape, BF16),
            dma((9,)),
            pltpu.VMEM((nt, length, x.shape[1]), BF16),
            pltpu.VMEM((w.shape[0], length), BF16),
            pltpu.VMEM((ny, 1, lanes), F32),
            pltpu.VMEM((nz, 1, lanes), F32),
        ]
        + scan_buffers()
        + scan_buffers()
        + [
            pltpu.VMEM((far + 1, ny, depth, WIDTH), BF16),
            pltpu.VMEM((ny, far + 1, depth, WIDTH), BF16),
            pltpu.VMEM((far + 1, depth, WIDTH), BF16),
            pltpu.VMEM((far, depth, WIDTH), BF16),
            pltpu.VMEM((near, ny, depth, WIDTH), BF16),
            pltpu.VMEM((near, ny, depth, WIDTH), BF16),
            pltpu.VMEM((ny, depth, WIDTH), BF16),
            pltpu.VMEM((ny, depth, WIDTH), BF16),
            dma((len(EXCHANGES),)),
            dma((len(EXCHANGES) + nt // 2,)),
        ],
        compiler_params=pltpu.CompilerParams(collective_id=0, has_side_effects=True),
    )(x, w, v, gf, gb, slack, extra.transpose(0, 2, 1), scale.reshape(1, WIDTH), cot)
    return pl.pallas_call(
        store,
        out_shape=tuple(jax.ShapeDtypeStruct(shape, dtype) for shape, dtype in results),
        in_specs=[vmem] * 5,
        out_specs=[anywhere] * 5,
        scratch_shapes=[dma((5,))],
    )(*(in_vmem(a) for a in held))


def solution(mesh):
    torus = Mesh(mesh.devices.reshape(NZ, NY, mesh.shape["tp"]), ("sp_0", "sp_1", "tp"))
    sp = ("sp_0", "sp_1")
    return jax.shard_map(
        functools.partial(on_device, NZ, NY),
        mesh=torus,
        in_specs=(
            P(sp, "tp"),
            P(None, "tp"),
            P(sp, "tp"),
            P(sp, "tp"),
            P(sp, "tp"),
            P(None, "tp"),
            P(None, sp, "tp"),
            P("tp"),
            P(sp, "tp"),
        ),
        out_specs=(P(sp, "tp"),) * 5,
        check_vma=False,
    )
```
